512 devices in a mesh: kv: 128 (over z, y, core), tp: 4 (over x).
Axes of the slice: x: 4, y: 8, z: 8, core: 2. Of those that a mesh axis runs over, the one named last changes fastest.
Arguments:
- tokens: bfloat16 [65536, 2048], P('kv'), may hold values from -18 to 18
- w_query: bfloat16 [2048, 1024], P(None, 'tp'), may hold values from -0.125 to 0.125
- w_key: bfloat16 [2048, 256], P(None, 'tp'), may hold values from -0.125 to 0.125
- w_value: bfloat16 [2048, 256], P(None, 'tp'), may hold values from -18 to 18
- w_out: bfloat16 [1024, 2048], P(None, 'tp'), may hold values from -0.1875 to 0.1875
- out_gain: float32 [1024], replicated, may hold values from 0.1 to 1.9
- chosen: int32 [4, 1024, 8], P('tp', 'kv'), may hold values from -1 to 1023, as said below
Outputs:
- mixed_out: bfloat16 [65536, 2048], P('kv', 'tp')
The draws below stay inside these ranges and needn't reach their ends.
Inputs may be any that keep to these rules, and one draw needn't show every extreme that they name: chosen[h, b, 0] is b itself; the other entries of a row are distinct key blocks lying wholly before block b, or -1, placed after all named blocks; for each key head h, the query blocks on one index of kv (its 512 positions) name, together, at most one key block of head h held by any other index of kv.
All inputs are finite; a program needn't handle non-finite values.
Results may differ from the reference program's by a relative error of at most 0.024.
Values may be sent and summed in bfloat16 or wider, within the bound.
A program may use at most 64 MiB of HBM per device.

```python
import jax
import jax.numpy as jnp
from jax import lax

D = 2048
HQ = 16
KVH = 4
HD = 64
BLK = 64
SEL = 8
TOK_DEV = 512
TOKENS = 65536
BLOCKS = 1024
N_KV = 128


def draw_tokens(key, part):
    return jax.random.truncated_normal(key, -6.0, 6.0, (TOKENS, D), jnp.float32).astype(jnp.bfloat16)


def draw_w_value(key, part):
    column_head = (jnp.arange(KVH * HD, dtype=jnp.int32) // HD).astype(jnp.float32)
    fraction = column_head / (KVH - 1)
    entries = jax.random.truncated_normal(key, -6.0, 6.0, (D, KVH * HD), jnp.float32)
    factor = 3.0 ** fraction
    return (entries * factor[None, :] * D ** (-0.5)).astype(jnp.bfloat16)


def draw_chosen(key, part):
    per_device = TOK_DEV // BLK
    extra = SEL - 1
    rank_total = min(N_KV, per_device * extra)
    key_one, key_two = jax.random.split(key)
    owner_pick = jax.random.randint(key_one, (KVH, N_KV, N_KV), 0, per_device)
    noise = jax.random.randint(key_two, (KVH, N_KV, N_KV), 0, 1024)
    device_ids = jnp.arange(N_KV, dtype=jnp.int32)[:, None]
    owner_ids = jnp.arange(N_KV, dtype=jnp.int32)[None, :]
    below = owner_ids < device_ids
    forced = below & ((owner_ids == device_ids - 1) | (owner_ids == device_ids - N_KV // 2) | (owner_ids == 0))
    ranking = (noise + 2048 * forced.astype(jnp.int32)[None]) * N_KV + (N_KV - 1 - owner_ids)[None]
    ranking = jnp.where(below[None], ranking, -1)
    ignored, order = lax.top_k(ranking, rank_total)
    block_ids = jnp.arange(BLOCKS, dtype=jnp.int32)
    device = block_ids // per_device
    local_index = block_ids % per_device
    slot = jnp.arange(extra, dtype=jnp.int32)[None, :]
    remote_count = jnp.clip(device - local_index * extra, 0, extra)[:, None]
    rank = jnp.minimum(local_index[:, None] * extra + slot, rank_total - 1)
    order_rows = order[:, device, :]
    owner_sel = jnp.take_along_axis(order_rows, jnp.broadcast_to(rank[None], (KVH, BLOCKS, extra)), axis=2)
    head_index = jnp.arange(KVH, dtype=jnp.int32)[:, None, None]
    candidate = owner_pick[head_index, device[None, :, None], owner_sel]
    remote_block = owner_sel * per_device + candidate
    local_slot = slot - remote_count
    local_block = device[:, None] * per_device + local_slot
    fallback = jnp.where((local_slot >= 0) & (local_slot < local_index[:, None]), local_block, -1)
    picked = jnp.where((slot < remote_count)[None], remote_block, fallback[None])
    own_block = jnp.broadcast_to(block_ids[None, :, None], (KVH, BLOCKS, 1))
    return jnp.concatenate([own_block, picked], axis=2).astype(jnp.int32)


def block_scale(key, dims, cuts, least, high):
    def one(dim, parts):
        draws = jax.random.uniform(jax.random.fold_in(jax.random.fold_in(key, 6), dim), (parts,), jnp.float32, least / len(cuts), high / len(cuts))
        return jnp.repeat(jnp.exp(draws), dims[dim] // parts).reshape((-1,) + (1,) * (len(dims) - dim - 1))

    factor_of = one(*cuts[0])
    for cut in cuts[1:]:
        factor_of = factor_of * one(*cut)
    return factor_of


def centred(rng, shape, width, most, shards=(), held_as=jnp.bfloat16):
    loudness = block_scale(rng, shape, shards, -0.22, 0.18) if shards else 1.0
    result = jax.random.normal(rng, shape, jnp.float32) * width * loudness
    return jnp.minimum(jnp.maximum(result, -most), most).astype(held_as)


def setup_inputs(seed: int = 0) -> dict:
    key_list = jax.random.split(jax.random.key(seed), 8)
    return {
        "tokens": draw_tokens(jax.random.fold_in(key_list[7], 71), 0),
        "w_query": centred(key_list[1], (D, HQ * HD), D ** -0.5, 0.125, ((1, 4),)),
        "w_key": centred(key_list[2], (D, KVH * HD), D ** -0.5, 0.125, ((1, 4),)),
        "w_value": draw_w_value(jax.random.fold_in(key_list[7], 71), 0),
        "w_out": centred(key_list[4], (HQ * HD, D), (HQ * HD) ** -0.5, 0.1875, ((1, 4),)),
        "out_gain": jnp.clip(1.0 + 0.18 * jax.random.normal(key_list[5], (HQ * HD,), jnp.float32), 0.1, 1.9),
        "chosen": draw_chosen(jax.random.fold_in(key_list[7], 71), 0),
    }


rope_base = 500000.0
norm_eps = 1e-06

def rotate(vectors, positions):
    half_size = vectors.shape[-1] // 2
    frequency = rope_base ** (-jnp.arange(half_size, dtype=jnp.float32) / half_size)
    angles = positions.astype(jnp.float32)[:, None] * frequency[None, :]
    cosine = jnp.cos(angles)[:, None, :]
    sine_wave = jnp.sin(angles)[:, None, :]
    lower_half = vectors[..., :half_size]
    upper_half = vectors[..., half_size:]
    return jnp.concatenate([lower_half * cosine - upper_half * sine_wave, upper_half * cosine + lower_half * sine_wave], axis=-1)

def reference(tokens, w_query, w_key, w_value, w_out, out_gain, chosen):
    row_total = tokens.shape[0]
    positions = jnp.arange(row_total, dtype=jnp.int32)
    queries = rotate(jnp.dot(tokens, w_query, preferred_element_type=jnp.float32).reshape(row_total, HQ, HD), positions).astype(jnp.bfloat16)
    key_rows = rotate(jnp.dot(tokens, w_key, preferred_element_type=jnp.float32).reshape(row_total, KVH, HD), positions).astype(jnp.bfloat16)
    value_rows = jnp.dot(tokens, w_value, preferred_element_type=jnp.float32).astype(jnp.bfloat16).reshape(row_total, KVH, HD)
    block_total = row_total // BLK
    group_size = HQ // KVH
    key_blocks = key_rows.reshape(block_total, BLK, KVH, HD).transpose(2, 0, 1, 3)
    value_blocks = value_rows.reshape(block_total, BLK, KVH, HD).transpose(2, 0, 1, 3)
    query_blocks = queries.reshape(block_total, BLK, KVH, group_size, HD)
    head_rows = jnp.arange(KVH, dtype=jnp.int32)[:, None]
    offsets = jnp.arange(BLK, dtype=jnp.int32)
    score_scale = HD ** (-0.5)

    def attend(block_index):
        chosen_ids = chosen[:, block_index, :]
        usable = chosen_ids >= 0
        safe_ids = jnp.maximum(chosen_ids, 0)
        key_part = key_blocks[head_rows, safe_ids].astype(jnp.float32)
        value_part = value_blocks[head_rows, safe_ids].astype(jnp.float32)
        query_part = query_blocks[block_index].astype(jnp.float32)
        scores = jnp.einsum('qhgd,hskd->hgqsk', query_part, key_part) * score_scale
        key_pos = chosen_ids[:, :, None] * BLK + offsets
        query_pos = block_index * BLK + offsets
        allowed = usable[:, None, :, None] & (key_pos[:, None, :, :] <= query_pos[None, :, None, None])
        scores = jnp.where(allowed[:, None], scores, -jnp.inf)
        peak_score = lax.optimization_barrier(jnp.max(scores, axis=(3, 4), keepdims=True))
        weights = jnp.exp(scores - peak_score)
        weights = weights / lax.optimization_barrier(jnp.sum(weights, axis=(3, 4), keepdims=True))
        weights = lax.optimization_barrier(weights.astype(jnp.bfloat16)).astype(jnp.float32)
        mixed_out = jnp.einsum('hgqsk,hskd->qhgd', weights, value_part)
        return mixed_out.reshape(BLK, HQ * HD).astype(jnp.bfloat16)
    attended = lax.map(attend, jnp.arange(block_total, dtype=jnp.int32)).reshape(row_total, HQ * HD)
    attn_f32 = attended.astype(jnp.float32)
    squares = lax.optimization_barrier(jnp.sum(attn_f32 * attn_f32, axis=1))
    inverse = lax.rsqrt(squares / (HQ * HD) + norm_eps)
    scaled = (attn_f32 * out_gain[None, :]).astype(jnp.bfloat16)
    product = jnp.dot(scaled, w_out, preferred_element_type=jnp.float32)
    return (inverse[:, None] * product).astype(jnp.bfloat16)
```

```python
import functools

import jax
import jax.numpy as jnp
from jax import lax
from jax.experimental import pallas as pl
from jax.experimental.pallas import tpu as pltpu
from jax.sharding import Mesh
from jax.sharding import PartitionSpec as P

HQ = 16
HD = 64
BLK = 64
SEL = 8
HALF = BLK // 2
CORES = 2
KV = ("kv_0", "kv_1", "kv_2")
MESH = pl.DeviceIdType.MESH

rope_base = 500000.0
norm_eps = 1e-06


def rope_tables(positions):
    half_size = HD // 2
    frequency = rope_base ** (-jnp.arange(half_size, dtype=jnp.float32) / half_size)
    angles = positions.astype(jnp.float32)[:, None] * frequency[None, :]
    return jnp.cos(angles)[:, None, :], jnp.sin(angles)[:, None, :]


def rotate(vectors, cosine, sine_wave):
    half_size = HD // 2
    lower_half = vectors[..., :half_size]
    upper_half = vectors[..., half_size:]
    return jnp.concatenate(
        [
            lower_half * cosine - upper_half * sine_wave,
            upper_half * cosine + lower_half * sine_wave,
        ],
        axis=-1,
    )


def exchange_kernel(
    nz, ny, chosen_ref, pairs_ref, ra_ref, rb_ref,
    ga, gb, sa, sb, want, wall, wsm,
    want_send, want_recv, smem_sem, own_sem, ring_send, ring_recv,
    a_send, a_recv, b_send, b_recv,
):
    z, y, c = lax.axis_index("kv_0"), lax.axis_index("kv_1"), lax.axis_index("kv_2")
    rows, cols = ny * CORES, nz * CORES
    row_me, col_me = y * CORES + c, z * CORES + c
    blocks = pairs_ref.shape[1]
    me = z * rows + row_me

    lane = lax.broadcasted_iota(jnp.int32, (blocks, 128), 1)
    found = jnp.full((blocks, 128), -1, jnp.int32)
    for s in range(SEL):
        ids = jnp.broadcast_to(chosen_ref[:, s : s + 1], (blocks, 128))
        hit = (ids // blocks == lane) & (ids >= 0) & (lane != me)
        found = jnp.maximum(found, jnp.where(hit, ids % blocks, -1))
    want[...] = jnp.max(found, axis=0, keepdims=True)

    def row_peer(d):
        p = lax.rem(row_me + d, rows)
        return p, {"kv_0": z, "kv_1": p // CORES, "kv_2": lax.rem(p, CORES)}

    def col_peer(d):
        p = lax.rem(col_me + d, cols)
        return p, {"kv_0": p // CORES, "kv_1": y, "kv_2": lax.rem(p, CORES)}

    barrier = pltpu.get_barrier_semaphore()

    @pl.loop(1, rows)
    def _(d):
        _, peer = row_peer(d)
        pl.semaphore_signal(barrier, inc=1, device_id=peer, device_id_type=MESH)

    @pl.loop(1, nz)
    def _(d):
        for core in range(CORES):
            peer = {"kv_0": lax.rem(z + d, nz), "kv_1": y, "kv_2": core}
            pl.semaphore_signal(barrier, inc=1, device_id=peer, device_id_type=MESH)

    pl.semaphore_wait(barrier, rows - 1 + (nz - 1) * CORES)

    own_a = pltpu.make_async_copy(pairs_ref.at[0], ga.at[z], own_sem.at[0])
    own_b = pltpu.make_async_copy(pairs_ref.at[1], gb.at[y], own_sem.at[1])
    own_a.start()
    own_b.start()
    pltpu.make_async_copy(want, wall.at[row_me], want_recv).start()
    pltpu.make_async_copy(want, wall.at[rows + col_me], want_recv).start()

    @pl.loop(1, rows)
    def _(d):
        _, peer = row_peer(d)
        pltpu.make_async_remote_copy(
            want, wall.at[row_me], want_send, want_recv, device_id=peer, device_id_type=MESH
        ).start()

    @pl.loop(1, cols)
    def _(d):
        _, peer = col_peer(d)
        pltpu.make_async_remote_copy(
            want, wall.at[rows + col_me], want_send, want_recv, device_id=peer, device_id_type=MESH
        ).start()

    def ring_copy(axis, way, step):
        name, place, size, held = (("kv_0", z, nz, ga), ("kv_1", y, ny, gb))[axis]
        if way == 0:
            source, target = lax.rem(place - step + size, size), lax.rem(place + 1, size)
        else:
            source, target = lax.rem(place + step, size), lax.rem(place + size - 1, size)
        return pltpu.make_async_remote_copy(
            pairs_ref.at[axis] if step == 0 else held.at[source],
            held.at[source],
            ring_send.at[axis, way, step],
            ring_recv.at[axis, way, step],
            device_id={name: target},
            device_id_type=MESH,
        )

    hops = {}
    for step in range(max(nz, ny) // 2 + 1):
        for axis, size in ((0, nz), (1, ny)):
            for way, count in ((0, size // 2), (1, (size - 1) // 2)):
                if 0 < step <= count:
                    hops[axis, way, step - 1].wait_recv()
                if step < count:
                    hops[axis, way, step] = ring_copy(axis, way, step)
                    hops[axis, way, step].start()
    own_a.wait()
    own_b.wait()

    pltpu.make_async_copy(wall, wall, want_recv).wait()
    to_smem = pltpu.make_async_copy(wall, wsm, smem_sem)
    to_smem.start()
    to_smem.wait()

    @pl.loop(0, rows)
    def _(p):
        for k in range(nz):
            block = jnp.maximum(wsm[p, 0, k * rows + row_me], 0)
            sa[p, k] = ga[k, block]

    @pl.loop(0, cols)
    def _(p):
        for k in range(ny):
            block = jnp.maximum(wsm[rows + p, 0, z * rows + k * CORES + c], 0)
            sb[p, k] = gb[k, block]

    keep_a = pltpu.make_async_copy(sa.at[row_me], ra_ref.at[row_me], a_recv.at[row_me])
    keep_b = pltpu.make_async_copy(sb.at[col_me], rb_ref.at[col_me], b_recv.at[col_me])
    keep_a.start()
    keep_b.start()

    def send_a(d):
        p, peer = row_peer(d)
        return pltpu.make_async_remote_copy(
            sa.at[p], ra_ref.at[row_me], a_send.at[p], a_recv.at[row_me],
            device_id=peer, device_id_type=MESH,
        )

    def send_b(d):
        p, peer = col_peer(d)
        copy = pltpu.make_async_remote_copy(
            sb.at[p], rb_ref.at[col_me], b_send.at[p], b_recv.at[col_me],
            device_id=peer, device_id_type=MESH,
        )
        return p // CORES >= z, copy

    @pl.loop(1, max(rows, cols))
    def _(d):
        if rows == cols:
            send_a(d).start()
        else:
            @pl.when(d < rows)
            def _():
                send_a(d).start()

        @pl.when(d < cols)
        def _():
            later, copy = send_b(d)

            @pl.when(later)
            def _():
                copy.start()

    for copy in hops.values():
        copy.wait_send()
    sends = wall.at[pl.ds(0, rows + cols - 2)]
    pltpu.make_async_copy(sends, sends, want_send).wait()

    @pl.loop(1, rows)
    def _(d):
        send_a(d).wait_send()

    @pl.loop(1, cols)
    def _(d):
        later, copy = send_b(d)

        @pl.when(later)
        def _():
            copy.wait_send()

    @pl.loop(0, rows)
    def _(p):
        pltpu.make_async_copy(sa.at[p], ra_ref.at[p], a_recv.at[p]).wait()

    @pl.loop(0, cols)
    def _(p):
        @pl.when(p // CORES <= z)
        def _():
            pltpu.make_async_copy(sb.at[p], rb_ref.at[p], b_recv.at[p]).wait()


def exchange(nz, ny, chosen, pairs):
    blocks = pairs.shape[1]
    rows, cols = ny * CORES, nz * CORES
    piece = (HALF, 2 * HD)
    vmem = pl.BlockSpec(memory_space=pltpu.VMEM)
    dma = pltpu.SemaphoreType.DMA
    return pl.pallas_call(
        functools.partial(exchange_kernel, nz, ny),
        out_shape=(
            jax.ShapeDtypeStruct((rows, nz, *piece), jnp.bfloat16),
            jax.ShapeDtypeStruct((cols, ny, *piece), jnp.bfloat16),
        ),
        in_specs=[vmem, vmem],
        out_specs=(vmem, vmem),
        scratch_shapes=[
            pltpu.VMEM((nz, blocks, *piece), jnp.bfloat16),
            pltpu.VMEM((ny, blocks, *piece), jnp.bfloat16),
            pltpu.VMEM((rows, nz, *piece), jnp.bfloat16),
            pltpu.VMEM((cols, ny, *piece), jnp.bfloat16),
            pltpu.VMEM((1, 128), jnp.int32),
            pltpu.VMEM((rows + cols, 1, 128), jnp.int32),
            pltpu.SMEM((rows + cols, 1, 128), jnp.int32),
            dma, dma, dma,
            dma((2,)),
            dma((2, 2, max(nz, ny) // 2)),
            dma((2, 2, max(nz, ny) // 2)),
            dma((rows,)),
            dma((rows,)),
            dma((cols,)),
            dma((cols,)),
        ],
        compiler_params=pltpu.CompilerParams(collective_id=0, has_side_effects=True),
    )(chosen, pairs)


def attend_kernel(
    nz, ny, nt, chosen_ref, q_ref, pairs_ref, ra_ref, rb_ref, w_ref, gain_ref, out_ref,
    kv, full, scaled_w, send_sem, recv_sem,
):
    z, y, c = lax.axis_index("kv_0"), lax.axis_index("kv_1"), lax.axis_index("kv_2")
    t = lax.axis_index("tp")
    rows = ny * CORES
    me = z * rows + y * CORES + c
    blocks = pairs_ref.shape[1]
    heads, row_count = q_ref.shape[0], q_ref.shape[1]
    chunk_blocks = 2
    chunks = blocks // chunk_blocks
    chunk_rows = chunk_blocks * BLK

    barrier = pltpu.get_barrier_semaphore()
    right, left = lax.rem(t + 1, nt), lax.rem(t + nt - 1, nt)
    across = lax.rem(t + 2, nt)
    for peer in (right, left):
        pl.semaphore_signal(barrier, inc=1, device_id={"tp": peer}, device_id_type=MESH)

    lane = lax.broadcasted_iota(jnp.int32, (1, SEL * BLK), 1)
    query_row = lax.broadcasted_iota(jnp.int32, (BLK, SEL * BLK), 0)
    key_col = lax.broadcasted_iota(jnp.int32, (BLK, SEL * BLK), 1)
    causal = jnp.where((key_col < BLK) & (key_col > query_row), -jnp.inf, 0.0).astype(jnp.float32)
    value_side = lax.broadcasted_iota(jnp.int32, (1, 2 * HD), 1) >= HD
    scaled_w[...] = (w_ref[...].astype(jnp.float32) * gain_ref[...]).astype(jnp.bfloat16)

    def attend_block(b):
        bias = jnp.zeros((1, SEL * BLK), jnp.float32)
        for s in range(SEL):
            named = chosen_ref[b, s]
            owner = lax.shift_right_arithmetic(named, 3)
            index = lax.bitwise_and(named, blocks - 1)
            here = (named < 0) | (owner == me)
            owner = jnp.where(here, me, owner)
            oz, oy, oc = owner // rows, lax.rem(owner, rows) // CORES, lax.rem(owner, CORES)
            kv[pl.ds(s * BLK, HALF)] = jnp.where(
                here, pairs_ref[0, index], ra_ref[oy * CORES + oc, oz]
            )
            kv[pl.ds(s * BLK + HALF, HALF)] = jnp.where(
                here, pairs_ref[1, index], rb_ref[oz * CORES + oc, oy]
            )
            if s > 0:
                bias = jnp.where((lane // BLK == s) & (named < 0), -jnp.inf, bias)
        keys = kv[...]
        first = b * BLK if isinstance(b, int) else pl.multiple_of(b * BLK, BLK)
        query = q_ref[:, pl.ds(first, BLK), :].reshape(heads * BLK, 2 * HD)
        scores = lax.dot_general(
            query, keys, (((1,), (1,)), ((), ())), preferred_element_type=jnp.float32
        )
        scores = scores.reshape(heads, BLK, SEL * BLK) + (causal + bias)[None]
        scores = scores.reshape(heads * BLK, SEL * BLK)
        peak = jnp.max(scores, axis=1, keepdims=True)
        weights = jnp.exp(scores - peak).astype(jnp.bfloat16)
        ones_or_values = jnp.where(value_side, keys, jnp.ones((), jnp.bfloat16))
        mixed = jnp.dot(weights, ones_or_values, preferred_element_type=jnp.float32)
        turned = pltpu.roll(mixed, HD, 1)
        outs = []
        for h in range(0, heads, 2):
            lo = slice(h * BLK, (h + 1) * BLK)
            hi = slice((h + 1) * BLK, (h + 2) * BLK)
            outs.append(
                jnp.where(value_side, mixed[hi], turned[lo])
                / jnp.where(value_side, turned[hi], mixed[lo])
            )
        return jnp.concatenate(outs, axis=1).astype(jnp.bfloat16)

    def piece(owner, k):
        return full.at[owner, pl.ds(k * chunk_rows, chunk_rows)]

    def near(way, k):
        return pltpu.make_async_remote_copy(
            piece(t, k), piece(t, k), send_sem.at[way, k], recv_sem.at[way, k],
            device_id={"tp": (right, left)[way]}, device_id_type=MESH,
        )

    def onward(k):
        way = k % 2
        source = (left, right)[way]
        return pltpu.make_async_remote_copy(
            piece(source, k), piece(source, k), send_sem.at[2, k], recv_sem.at[2, k],
            device_id={"tp": (right, left)[way]}, device_id_type=MESH,
        )

    for k in range(chunks):
        for i in range(chunk_blocks):
            b = k * chunk_blocks + i
            full[t, pl.ds(b * BLK, BLK)] = attend_block(b)
        if k == 0:
            pl.semaphore_wait(barrier, 2)
        near(0, k).start()
        near(1, k).start()
        if k > 0:
            near((k - 1) % 2, k - 1).wait_recv()
            onward(k - 1).start()
    near((chunks - 1) % 2, chunks - 1).wait_recv()
    onward(chunks - 1).start()

    width = heads * HD
    for k in range(chunks):
        near((k + 1) % 2, k).wait_recv()
        onward(k).wait_recv()
        total = None
        squares = None
        for owner in range(nt):
            part = full[owner, pl.ds(k * chunk_rows, chunk_rows)]
            wide = part.astype(jnp.float32)
            square = jnp.sum(wide * wide, axis=1, keepdims=True)
            term = jnp.dot(
                part,
                scaled_w[pl.ds(owner * width, width), :],
                preferred_element_type=jnp.float32,
            )
            total = term if total is None else total + term
            squares = square if squares is None else squares + square
        inverse = lax.rsqrt(squares / (HQ * HD) + norm_eps)
        out_ref[pl.ds(k * chunk_rows, chunk_rows), :] = (inverse * total).astype(jnp.bfloat16)
    for k in range(chunks):
        near(0, k).wait_send()
        near(1, k).wait_send()
        onward(k).wait_send()


def attend(nz, ny, nt, chosen, queries, pairs, ra, rb, w_out, gain):
    heads, row_count = queries.shape[:2]
    vmem = pl.BlockSpec(memory_space=pltpu.VMEM)
    chunks = pairs.shape[1] // 2
    return pl.pallas_call(
        functools.partial(attend_kernel, nz, ny, nt),
        out_shape=jax.ShapeDtypeStruct((row_count, w_out.shape[1]), jnp.bfloat16),
        in_specs=[pl.BlockSpec(memory_space=pltpu.SMEM)] + [vmem] * 6,
        out_specs=vmem,
        scratch_shapes=[
            pltpu.VMEM((SEL * BLK, 2 * HD), jnp.bfloat16),
            pltpu.VMEM((nt, row_count, heads * HD), jnp.bfloat16),
            pltpu.VMEM(w_out.shape, jnp.bfloat16),
            pltpu.SemaphoreType.DMA((3, chunks)),
            pltpu.SemaphoreType.DMA((3, chunks)),
        ],
        compiler_params=pltpu.CompilerParams(collective_id=1, has_side_effects=True),
    )(chosen, queries, pairs, ra, rb, w_out, gain)


def per_device(tokens, w_query, w_key, w_value, w_out, out_gain, chosen):
    nz, ny, nt = lax.axis_size("kv_0"), lax.axis_size("kv_1"), lax.axis_size("tp")
    kv_place = lax.axis_index(KV)
    row_count = tokens.shape[0]
    block_count = row_count // BLK
    head_count = w_query.shape[1] // HD
    positions = kv_place * row_count + jnp.arange(row_count, dtype=jnp.int32)
    cosine, sine_wave = rope_tables(positions)
    w_pair = jnp.concatenate([w_key, w_value], axis=1)
    pair = jnp.dot(tokens, w_pair, preferred_element_type=jnp.float32)
    key_rows = rotate(pair[:, None, :HD], cosine, sine_wave)[:, 0]
    pairs = jnp.concatenate([key_rows, pair[:, HD:]], axis=1).astype(jnp.bfloat16)
    pairs = pairs.reshape(block_count, 2, HALF, 2 * HD).transpose(1, 0, 2, 3)
    chosen_ids = chosen[0]
    ra, rb = exchange(nz, ny, chosen_ids, pairs)
    queries = rotate(
        jnp.dot(tokens, w_query, preferred_element_type=jnp.float32).reshape(
            row_count, head_count, HD
        ),
        cosine,
        sine_wave,
    ).astype(jnp.bfloat16) * jnp.bfloat16(HD ** (-0.5))
    queries = jnp.pad(queries.transpose(1, 0, 2), ((0, 0), (0, 0), (0, HD)))
    return attend(nz, ny, nt, chosen_ids, queries, pairs, ra, rb, w_out, out_gain[:, None])


def solution(mesh):
    count = mesh.shape["kv"]
    ny = 8 if count == 128 else 2
    nz = count // (ny * CORES)
    finer = Mesh(
        mesh.devices.reshape(nz, ny, CORES, mesh.shape["tp"]), ("kv_0", "kv_1", "kv_2", "tp")
    )
    placed = (
        P(KV, None),
        P(None, "tp"),
        P(None, "tp"),
        P(None, "tp"),
        P(None, "tp"),
        P(),
        P("tp", KV, None),
    )
    return jax.shard_map(
        per_device, mesh=finer, in_specs=placed, out_specs=P(KV, "tp"), check_vma=False
    )
```

```python
import functools

import jax
import jax.numpy as jnp
from jax import lax
from jax.experimental import pallas as pl
from jax.experimental.pallas import tpu as pltpu
from jax.sharding import Mesh
from jax.sharding import PartitionSpec as P

HQ = 16
HD = 64
BLK = 64
SEL = 8
HALF = BLK // 2
CORES = 2
KV = ("kv_0", "kv_1", "kv_2")
MESH = pl.DeviceIdType.MESH

rope_base = 500000.0
norm_eps = 1e-06


def layer_kernel(
    nz, ny, nt,
    ids_ref, chosen_ref, table_ref, gain_ref, tokens_hbm, wk_hbm, wv_hbm, wq_hbm, wo_hbm, out_ref,
    tokens, w_pair, w_query, w_out, pairs, query, ga, gb, sa, sb, ra, rb, want, wall, wsm, kv, full,
    load_sem, want_send, want_recv, smem_sem, ring_send, ring_recv,
    a_send, a_recv, b_send, b_recv, tp_send, tp_recv,
):
    z, y, c = lax.axis_index("kv_0"), lax.axis_index("kv_1"), lax.axis_index("kv_2")
    t = lax.axis_index("tp")
    rows, cols = ny * CORES, nz * CORES
    row_me, col_me = y * CORES + c, z * CORES + c
    blocks = pairs.shape[1]
    me = z * rows + row_me
    heads = query.shape[0]

    def row_peer(d):
        p = lax.rem(row_me + d, rows)
        return p, {"kv_0": z, "kv_1": p // CORES, "kv_2": lax.rem(p, CORES)}

    def col_peer(d):
        p = lax.rem(col_me + d, cols)
        return p, {"kv_0": p // CORES, "kv_1": y, "kv_2": lax.rem(p, CORES)}

    right, left = lax.rem(t + 1, nt), lax.rem(t + nt - 1, nt)
    barrier = pltpu.get_barrier_semaphore()

    @pl.loop(1, rows)
    def _(d):
        _, peer = row_peer(d)
        pl.semaphore_signal(barrier, inc=1, device_id=peer, device_id_type=MESH)

    @pl.loop(1, nz)
    def _(d):
        for core in range(CORES):
            peer = {"kv_0": lax.rem(z + d, nz), "kv_1": y, "kv_2": core}
            pl.semaphore_signal(barrier, inc=1, device_id=peer, device_id_type=MESH)

    for peer in (right, left):
        pl.semaphore_signal(barrier, inc=1, device_id={"tp": peer}, device_id_type=MESH)

    loads = [
        pltpu.make_async_copy(wk_hbm, w_pair.at[pl.ds(0, HD)], load_sem.at[0]),
        pltpu.make_async_copy(wv_hbm, w_pair.at[pl.ds(HD, HD)], load_sem.at[1]),
        pltpu.make_async_copy(tokens_hbm, tokens, load_sem.at[2]),
        pltpu.make_async_copy(wq_hbm, w_query, load_sem.at[3]),
        pltpu.make_async_copy(wo_hbm, w_out, load_sem.at[4]),
    ]
    for load in loads:
        load.start()

    lane = lax.broadcasted_iota(jnp.int32, (blocks, 128), 1)
    found = jnp.full((blocks, 128), -1, jnp.int32)
    for s in range(SEL):
        ids = jnp.broadcast_to(ids_ref[:, s : s + 1], (blocks, 128))
        hit = (ids // blocks == lane) & (ids >= 0) & (lane != me)
        found = jnp.maximum(found, jnp.where(hit, ids % blocks, -1))
    want[...] = jnp.max(found, axis=0, keepdims=True)

    head_lane = lax.broadcasted_iota(jnp.int32, (1, 2 * HD), 1)
    value_side = head_lane >= HD
    lower_side = head_lane % HD < HD // 2

    def turned(wide, b, only_keys):
        cos_row, sin_row = table_ref[0, pl.ds(0, BLK)], table_ref[1, pl.ds(0, BLK)]
        cos_base, sin_base = table_ref[0, pl.ds(BLK + b, 1)], table_ref[1, pl.ds(BLK + b, 1)]
        cosine = cos_base * cos_row - sin_base * sin_row
        sine_wave = sin_base * cos_row + cos_base * sin_row
        if only_keys:
            cosine = jnp.where(value_side, 1.0, cosine)
            sine_wave = jnp.where(value_side, 0.0, sine_wave)
        other = jnp.where(lower_side, pltpu.roll(wide, 3 * HD // 2, 1), pltpu.roll(wide, HD // 2, 1))
        return wide * cosine + other * sine_wave

    for load in loads[:3]:
        load.wait()
    pair = lax.dot_general(
        tokens[...], w_pair[...], (((1,), (1,)), ((), ())), preferred_element_type=jnp.float32
    )
    for b in range(blocks):
        held = turned(pair[b * BLK : (b + 1) * BLK], b, True).astype(jnp.bfloat16)
        pairs[0, b] = held[:HALF]
        pairs[1, b] = held[HALF:]

    pl.semaphore_wait(barrier, rows - 1 + (nz - 1) * CORES + 2)

    pltpu.make_async_copy(want, wall.at[row_me], want_recv).start()
    pltpu.make_async_copy(want, wall.at[rows + col_me], want_recv).start()

    @pl.loop(1, rows)
    def _(d):
        _, peer = row_peer(d)
        pltpu.make_async_remote_copy(
            want, wall.at[row_me], want_send, want_recv, device_id=peer, device_id_type=MESH
        ).start()

    @pl.loop(1, cols)
    def _(d):
        _, peer = col_peer(d)
        pltpu.make_async_remote_copy(
            want, wall.at[rows + col_me], want_send, want_recv, device_id=peer, device_id_type=MESH
        ).start()

    def ring_copy(axis, way, step):
        name, place, size, held = (("kv_0", z, nz, ga), ("kv_1", y, ny, gb))[axis]
        target = lax.rem(place + (1, size - 1)[way], size)
        return pltpu.make_async_remote_copy(
            pairs.at[axis] if step == 0 else held[2 * step - 2 + way],
            held[2 * step + way],
            ring_send.at[axis, way, step],
            ring_recv.at[axis, way, step],
            device_id={name: target},
            device_id_type=MESH,
        )

    def source_of(place, size, k):
        if k % 2:
            return lax.rem(place - (k + 1) // 2 + size, size)
        return lax.rem(place + k // 2, size)

    def groups_of(size):
        found = [(0, 1)]
        for s in range(1, size // 2 + 1):
            found.append((2 * s - 1, min(2 * s + 1, size)))
        if size >= 8:
            found[-2:] = [(found[-2][0], found[-1][1])]
        return found

    def ready_at(size, group):
        return group[1] // 2

    groups_a, groups_b = groups_of(nz), groups_of(ny)

    def send_a(d, g):
        p, peer = row_peer(d)
        lo, hi = groups_a[g]
        part = pl.ds(lo, hi - lo)
        return pltpu.make_async_remote_copy(
            sa.at[p, part], ra.at[row_me, part], a_send.at[g, p], a_recv.at[g, row_me],
            device_id=peer, device_id_type=MESH,
        )

    def send_b(d, g):
        p, peer = col_peer(d)
        lo, hi = groups_b[g]
        part = pl.ds(lo, hi - lo)
        copy = pltpu.make_async_remote_copy(
            sb.at[p, part], rb.at[col_me, part], b_send.at[g, p], b_recv.at[g, col_me],
            device_id=peer, device_id_type=MESH,
        )
        return p // CORES >= z, copy

    def needed_a(g):
        return z >= (groups_a[g][0] + 1) // 2

    def select_a(g):
        @pl.when(needed_a(g))
        def _():
            @pl.loop(0, rows)
            def _(p):
                for k in range(*groups_a[g]):
                    source = source_of(z, nz, k)
                    block = jnp.maximum(wsm[p, 0, source * rows + row_me], 0)
                    sa[p, k] = pairs[0, block] if k == 0 else ga[k - 1][block]

    def select_b(g):
        @pl.loop(0, cols)
        def _(p):
            for k in range(*groups_b[g]):
                source = source_of(y, ny, k)
                block = jnp.maximum(wsm[rows + p, 0, z * rows + source * CORES + c], 0)
                sb[p, k] = pairs[1, block] if k == 0 else gb[k - 1][block]

    def start_a(g):
        lo, hi = groups_a[g]
        part = pl.ds(lo, hi - lo)

        @pl.when(needed_a(g))
        def _():
            @pl.loop(1, rows)
            def _(d):
                send_a(d, g).start()

            pltpu.make_async_copy(
                sa.at[row_me, part], ra.at[row_me, part], a_recv.at[g, row_me]
            ).start()

    def start_b(g):
        lo, hi = groups_b[g]
        part = pl.ds(lo, hi - lo)

        @pl.loop(1, cols)
        def _(d):
            later, copy = send_b(d, g)

            @pl.when(later)
            def _():
                copy.start()

        pltpu.make_async_copy(
            sb.at[col_me, part], rb.at[col_me, part], b_recv.at[g, col_me]
        ).start()

    hops = {}
    for step in range(max(nz, ny) // 2 + 1):
        for axis, size in ((0, nz), (1, ny)):
            for way, count in ((0, size // 2), (1, (size - 1) // 2)):
                if 0 < step <= count:
                    hops[axis, way, step - 1].wait_recv()
                if step < count:
                    hops[axis, way, step] = ring_copy(axis, way, step)
                    hops[axis, way, step].start()
        if step == 0:
            loads[3].wait()
            product = jnp.dot(tokens[...], w_query[...], preferred_element_type=jnp.float32)
            for b in range(blocks):
                for h in range(0, heads, 2):
                    wide = product[b * BLK : (b + 1) * BLK, h * HD : (h + 2) * HD]
                    wide = turned(wide, b, False) * (HD ** -0.5)
                    spot = pl.ds(b * BLK, BLK)
                    query[h, spot] = jnp.where(value_side, 0.0, wide).astype(jnp.bfloat16)
                    query[h + 1, spot] = jnp.where(
                        value_side, 0.0, pltpu.roll(wide, HD, 1)
                    ).astype(jnp.bfloat16)
            pltpu.make_async_copy(wall, wall, want_recv).wait()
            to_smem = pltpu.make_async_copy(wall, wsm, smem_sem)
            to_smem.start()
            to_smem.wait()
        now_a = [g for g, group in enumerate(groups_a) if ready_at(nz, group) == step]
        now_b = [g for g, group in enumerate(groups_b) if ready_at(ny, group) == step]
        for g in now_a:
            select_a(g)
        for g in now_b:
            select_b(g)
        for g in now_a:
            start_a(g)
        for g in now_b:
            start_b(g)

    loads[4].wait()

    @pl.loop(0, rows)
    def _(p):
        for g, (lo, hi) in enumerate(groups_a):
            part = pl.ds(lo, hi - lo)

            @pl.when(needed_a(g))
            def _():
                pltpu.make_async_copy(sa.at[p, part], ra.at[p, part], a_recv.at[g, p]).wait()

    @pl.loop(0, cols)
    def _(p):
        @pl.when(p // CORES <= z)
        def _():
            for g, (lo, hi) in enumerate(groups_b):
                part = pl.ds(lo, hi - lo)
                pltpu.make_async_copy(sb.at[p, part], rb.at[p, part], b_recv.at[g, p]).wait()

    chunk_blocks = 2
    chunks = blocks // chunk_blocks
    chunk_rows = chunk_blocks * BLK
    key_lane = lax.broadcasted_iota(jnp.int32, (1, SEL * BLK), 1)
    query_row = lax.broadcasted_iota(jnp.int32, (BLK, SEL * BLK), 0)
    key_col = lax.broadcasted_iota(jnp.int32, (BLK, SEL * BLK), 1)
    causal = jnp.where((key_col < BLK) & (key_col > query_row), -jnp.inf, 0.0).astype(jnp.float32)

    def slot_of(place, size, owner):
        r = lax.rem(place - owner + size, size)
        return jnp.where(r <= size // 2, jnp.maximum(2 * r - 1, 0), 2 * (size - r))

    def attend_block(b):
        bias = jnp.zeros((1, SEL * BLK), jnp.float32)
        for s in range(SEL):
            named = chosen_ref[b, s]
            owner = lax.shift_right_arithmetic(named, 3)
            index = lax.bitwise_and(named, blocks - 1)
            here = (named < 0) | (owner == me)
            owner = jnp.where(here, me, owner)
            oz, oy, oc = owner // rows, lax.rem(owner, rows) // CORES, lax.rem(owner, CORES)
            kv[pl.ds(s * BLK, HALF)] = jnp.where(
                here, pairs[0, index], ra[oy * CORES + oc, slot_of(z, nz, oz)]
            )
            kv[pl.ds(s * BLK + HALF, HALF)] = jnp.where(
                here, pairs[1, index], rb[oz * CORES + oc, slot_of(y, ny, oy)]
            )
            if s > 0:
                bias = jnp.where((key_lane // BLK == s) & (named < 0), -jnp.inf, bias)
        keys = kv[...]
        queries = query[:, pl.ds(b * BLK, BLK), :].reshape(heads * BLK, 2 * HD)
        scores = lax.dot_general(
            queries, keys, (((1,), (1,)), ((), ())), preferred_element_type=jnp.float32
        )
        scores = scores.reshape(heads, BLK, SEL * BLK) + (causal + bias)[None]
        scores = scores.reshape(heads * BLK, SEL * BLK)
        peak = jnp.max(scores, axis=1, keepdims=True)
        weights = jnp.exp(scores - peak).astype(jnp.bfloat16)
        ones_or_values = jnp.where(value_side, keys, jnp.ones((), jnp.bfloat16))
        mixed = jnp.dot(weights, ones_or_values, preferred_element_type=jnp.float32)
        swapped = pltpu.roll(mixed, HD, 1)
        outs = []
        for h in range(0, heads, 2):
            lo = slice(h * BLK, (h + 1) * BLK)
            hi = slice((h + 1) * BLK, (h + 2) * BLK)
            outs.append(
                jnp.where(value_side, mixed[hi], swapped[lo])
                / jnp.where(value_side, swapped[hi], mixed[lo])
            )
        return jnp.concatenate(outs, axis=1).astype(jnp.bfloat16)

    def piece(owner, k):
        return full.at[owner, pl.ds(k * chunk_rows, chunk_rows)]

    def near(way, k):
        return pltpu.make_async_remote_copy(
            piece(t, k), piece(t, k), tp_send.at[way, k], tp_recv.at[way, k],
            device_id={"tp": (right, left)[way]}, device_id_type=MESH,
        )

    def onward(k):
        way = k % 2
        source = (left, right)[way]
        return pltpu.make_async_remote_copy(
            piece(source, k), piece(source, k), tp_send.at[2, k], tp_recv.at[2, k],
            device_id={"tp": (right, left)[way]}, device_id_type=MESH,
        )

    for k in range(chunks):
        for i in range(chunk_blocks):
            b = k * chunk_blocks + i
            full[t, pl.ds(b * BLK, BLK)] = attend_block(b)
        near(0, k).start()
        near(1, k).start()
        if k > 0:
            near((k - 1) % 2, k - 1).wait_recv()
            onward(k - 1).start()
    near((chunks - 1) % 2, chunks - 1).wait_recv()
    onward(chunks - 1).start()

    width = heads * HD
    for k in range(chunks):
        near((k + 1) % 2, k).wait_recv()
        onward(k).wait_recv()
        total = None
        squares = None
        for owner in range(nt):
            wide = full[owner, pl.ds(k * chunk_rows, chunk_rows)].astype(jnp.float32)
            square = jnp.sum(wide * wide, axis=1, keepdims=True)
            scaled = (wide * gain_ref[:, pl.ds(owner * width, width)]).astype(jnp.bfloat16)
            term = jnp.dot(
                scaled,
                w_out[pl.ds(owner * width, width), :],
                preferred_element_type=jnp.float32,
            )
            total = term if total is None else total + term
            squares = square if squares is None else squares + square
        inverse = lax.rsqrt(squares / (HQ * HD) + norm_eps)
        out_ref[pl.ds(k * chunk_rows, chunk_rows), :] = (inverse * total).astype(jnp.bfloat16)

    for copy in hops.values():
        copy.wait_send()
    sends = wall.at[pl.ds(0, rows + cols - 2)]
    pltpu.make_async_copy(sends, sends, want_send).wait()

    @pl.loop(1, rows)
    def _(d):
        for g in range(len(groups_a)):
            @pl.when(needed_a(g))
            def _():
                send_a(d, g).wait_send()

    @pl.loop(1, cols)
    def _(d):
        for g in range(len(groups_b)):
            later, copy = send_b(d, g)

            @pl.when(later)
            def _():
                copy.wait_send()

    for k in range(chunks):
        near(0, k).wait_send()
        near(1, k).wait_send()
        onward(k).wait_send()


def per_device(tokens, w_query, w_key, w_value, w_out, out_gain, chosen):
    nz, ny, nt = lax.axis_size("kv_0"), lax.axis_size("kv_1"), lax.axis_size("tp")
    kv_place = lax.axis_index(KV)
    row_count, depth = tokens.shape
    blocks = row_count // BLK
    heads = w_query.shape[1] // HD
    rows, cols = ny * CORES, nz * CORES
    half_size = HD // 2
    frequency = rope_base ** (-jnp.arange(half_size, dtype=jnp.float32) / half_size)
    places = jnp.concatenate(
        [
            jnp.arange(BLK, dtype=jnp.int32),
            kv_place * row_count + BLK * jnp.arange(blocks, dtype=jnp.int32),
        ]
    )
    angles = places.astype(jnp.float32)[:, None] * jnp.tile(frequency, 4)[None, :]
    sign = jnp.where(jnp.arange(2 * HD) % HD < half_size, -1.0, 1.0)
    table = jnp.stack([jnp.cos(angles), jnp.sin(angles) * sign])

    piece = (HALF, 2 * HD)
    vmem = pl.BlockSpec(memory_space=pltpu.VMEM)
    far = pl.BlockSpec(memory_space=pl.ANY)
    dma = pltpu.SemaphoreType.DMA
    bf16 = jnp.bfloat16
    steps = max(nz, ny) // 2
    return pl.pallas_call(
        functools.partial(layer_kernel, nz, ny, nt),
        out_shape=jax.ShapeDtypeStruct((row_count, w_out.shape[1]), bf16),
        in_specs=[vmem, pl.BlockSpec(memory_space=pltpu.SMEM), vmem, vmem] + [far] * 5,
        out_specs=vmem,
        scratch_shapes=[
            pltpu.VMEM((row_count, depth), bf16),
            pltpu.VMEM((2 * HD, depth), bf16),
            pltpu.VMEM(w_query.shape, bf16),
            pltpu.VMEM(w_out.shape, bf16),
            pltpu.VMEM((2, blocks, *piece), bf16),
            pltpu.VMEM((heads, row_count, 2 * HD), bf16),
            [pltpu.VMEM((blocks, *piece), bf16)] * (nz - 1),
            [pltpu.VMEM((blocks, *piece), bf16)] * (ny - 1),
            pltpu.VMEM((rows, nz, *piece), bf16),
            pltpu.VMEM((cols, ny, *piece), bf16),
            pltpu.VMEM((rows, nz, *piece), bf16),
            pltpu.VMEM((cols, ny, *piece), bf16),
            pltpu.VMEM((1, 128), jnp.int32),
            pltpu.VMEM((rows + cols, 1, 128), jnp.int32),
            pltpu.SMEM((rows + cols, 1, 128), jnp.int32),
            pltpu.VMEM((SEL * BLK, 2 * HD), bf16),
            pltpu.VMEM((nt, row_count, heads * HD), bf16),
            dma((5,)),
            dma, dma, dma,
            dma((2, 2, steps)),
            dma((2, 2, steps)),
            dma((4, rows)),
            dma((4, rows)),
            dma((4, cols)),
            dma((4, cols)),
            dma((3, blocks // 2)),
            dma((3, blocks // 2)),
        ],
        compiler_params=pltpu.CompilerParams(collective_id=0, has_side_effects=True),
    )(
        chosen[0], chosen[0], table, out_gain[None, :],
        tokens, w_key.T, w_value.T, w_query, w_out,
    )


def solution(mesh):
    count = mesh.shape["kv"]
    ny = 8 if count == 128 else 2
    nz = count // (ny * CORES)
    finer = Mesh(
        mesh.devices.reshape(nz, ny, CORES, mesh.shape["tp"]), ("kv_0", "kv_1", "kv_2", "tp")
    )
    placed = (
        P(KV, None),
        P(None, "tp"),
        P(None, "tp"),
        P(None, "tp"),
        P(None, "tp"),
        P(),
        P("tp", KV, None),
    )
    return jax.shard_map(
        per_device, mesh=finer, in_specs=placed, out_specs=P(KV, "tp"), check_vma=False
    )
```

```python
import functools

import jax
import jax.numpy as jnp
from jax import lax
from jax.experimental import pallas as pl
from jax.experimental.pallas import tpu as pltpu
from jax.sharding import Mesh
from jax.sharding import PartitionSpec as P

HQ = 16
HD = 64
BLK = 64
SEL = 8
HALF = BLK // 2
CORES = 2
KV = ("kv_0", "kv_1", "kv_2")
MESH = pl.DeviceIdType.MESH

rope_base = 500000.0
norm_eps = 1e-06


def layer_kernel(
    nz, ny, nt,
    ids_ref, chosen_ref, table_ref, gain_ref, tokens_hbm, wk_hbm, wv_hbm, wq_hbm, wo_hbm, out_ref,
    tokens, w_pair, w_query, w_out, pairs, query, ga, gb, sa, sb, ra, rb, want, wall, wsm, kv, full,
    load_sem, want_send, want_recv, smem_sem, ring_send, ring_recv,
    a_send, a_recv, b_send, b_recv, tp_send, tp_recv,
):
    z, y, c = lax.axis_index("kv_0"), lax.axis_index("kv_1"), lax.axis_index("kv_2")
    t = lax.axis_index("tp")
    rows, cols = ny * CORES, nz * CORES
    row_me, col_me = y * CORES + c, z * CORES + c
    blocks = pairs.shape[1]
    me = z * rows + row_me
    heads, row_count = query.shape[0], query.shape[1]

    def row_peer(d):
        p = lax.rem(row_me + d, rows)
        return p, {"kv_0": z, "kv_1": p // CORES, "kv_2": lax.rem(p, CORES)}

    def col_peer(d):
        p = lax.rem(col_me + d, cols)
        return p, {"kv_0": p // CORES, "kv_1": y, "kv_2": lax.rem(p, CORES)}

    right, left = lax.rem(t + 1, nt), lax.rem(t + nt - 1, nt)
    barrier = pltpu.get_barrier_semaphore()

    @pl.loop(1, rows)
    def _(d):
        _, peer = row_peer(d)
        pl.semaphore_signal(barrier, inc=1, device_id=peer, device_id_type=MESH)

    @pl.loop(1, nz)
    def _(d):
        for core in range(CORES):
            peer = {"kv_0": lax.rem(z + d, nz), "kv_1": y, "kv_2": core}
            pl.semaphore_signal(barrier, inc=1, device_id=peer, device_id_type=MESH)

    for peer in (right, left):
        pl.semaphore_signal(barrier, inc=1, device_id={"tp": peer}, device_id_type=MESH)

    loads = [
        pltpu.make_async_copy(wk_hbm, w_pair.at[pl.ds(0, HD)], load_sem.at[0]),
        pltpu.make_async_copy(wv_hbm, w_pair.at[pl.ds(HD, HD)], load_sem.at[1]),
        pltpu.make_async_copy(tokens_hbm, tokens, load_sem.at[2]),
        pltpu.make_async_copy(wq_hbm, w_query, load_sem.at[3]),
        pltpu.make_async_copy(wo_hbm, w_out, load_sem.at[4]),
    ]
    for load in loads:
        load.start()

    lane = lax.broadcasted_iota(jnp.int32, (blocks, 128), 1)
    found = jnp.full((blocks, 128), -1, jnp.int32)
    for s in range(SEL):
        ids = jnp.broadcast_to(ids_ref[:, s : s + 1], (blocks, 128))
        hit = (ids // blocks == lane) & (ids >= 0) & (lane != me)
        found = jnp.maximum(found, jnp.where(hit, ids % blocks, -1))
    want[...] = jnp.max(found, axis=0, keepdims=True)

    head_lane = lax.broadcasted_iota(jnp.int32, (1, 2 * HD), 1)
    value_side = head_lane >= HD
    lower_side = head_lane % HD < HD // 2

    def turned(wide, b, only_keys):
        cos_row, sin_row = table_ref[0, pl.ds(0, BLK)], table_ref[1, pl.ds(0, BLK)]
        cos_base, sin_base = table_ref[0, pl.ds(BLK + b, 1)], table_ref[1, pl.ds(BLK + b, 1)]
        cosine = cos_base * cos_row - sin_base * sin_row
        sine_wave = sin_base * cos_row + cos_base * sin_row
        if only_keys:
            cosine = jnp.where(value_side, 1.0, cosine)
            sine_wave = jnp.where(value_side, 0.0, sine_wave)
        other = jnp.where(lower_side, pltpu.roll(wide, 3 * HD // 2, 1), pltpu.roll(wide, HD // 2, 1))
        return wide * cosine + other * sine_wave

    for load in loads[:3]:
        load.wait()
    pair = lax.dot_general(
        tokens[...], w_pair[...], (((1,), (1,)), ((), ())), preferred_element_type=jnp.float32
    )
    for b in range(blocks):
        held = turned(pair[b * BLK : (b + 1) * BLK], b, True).astype(jnp.bfloat16)
        pairs[0, b] = held[:HALF]
        pairs[1, b] = held[HALF:]

    pl.semaphore_wait(barrier, rows - 1 + (nz - 1) * CORES + 2)

    pltpu.make_async_copy(want, wall.at[row_me], want_recv).start()
    pltpu.make_async_copy(want, wall.at[rows + col_me], want_recv).start()

    @pl.loop(1, rows)
    def _(d):
        _, peer = row_peer(d)
        pltpu.make_async_remote_copy(
            want, wall.at[row_me], want_send, want_recv, device_id=peer, device_id_type=MESH
        ).start()

    @pl.loop(1, cols)
    def _(d):
        _, peer = col_peer(d)
        pltpu.make_async_remote_copy(
            want, wall.at[rows + col_me], want_send, want_recv, device_id=peer, device_id_type=MESH
        ).start()

    def ring_copy(axis, way, step):
        name, place, size, held = (("kv_0", z, nz, ga), ("kv_1", y, ny, gb))[axis]
        target = lax.rem(place + (1, size - 1)[way], size)
        return pltpu.make_async_remote_copy(
            pairs.at[axis] if step == 0 else held[2 * step - 2 + way],
            held[2 * step + way],
            ring_send.at[axis, way, step],
            ring_recv.at[axis, way, step],
            device_id={name: target},
            device_id_type=MESH,
        )

    def source_of(place, size, k):
        if k % 2:
            return lax.rem(place - (k + 1) // 2 + size, size)
        return lax.rem(place + k // 2, size)

    def groups_of(size):
        found = [(0, 1)]
        for s in range(1, size // 2 + 1):
            found.append((2 * s - 1, min(2 * s + 1, size)))
        if size >= 8:
            found[-2:] = [(found[-2][0], found[-1][1])]
        return found

    def sent_at(group):
        return min(group[1] // 2 + 1, last)

    groups_a, groups_b = groups_of(nz), groups_of(ny)

    def send_a(d, g):
        p, peer = row_peer(d)
        lo, hi = groups_a[g]
        part = pl.ds(lo, hi - lo)
        return pltpu.make_async_remote_copy(
            sa.at[p, part], ra.at[row_me, part], a_send.at[g, p], a_recv.at[g, row_me],
            device_id=peer, device_id_type=MESH,
        )

    def send_b(d, g):
        p, peer = col_peer(d)
        lo, hi = groups_b[g]
        part = pl.ds(lo, hi - lo)
        copy = pltpu.make_async_remote_copy(
            sb.at[p, part], rb.at[col_me, part], b_send.at[g, p], b_recv.at[g, col_me],
            device_id=peer, device_id_type=MESH,
        )
        return p // CORES >= z, copy

    def needed_a(g):
        return z >= (groups_a[g][0] + 1) // 2

    def select_a(g):
        @pl.when(needed_a(g))
        def _():
            @pl.loop(0, rows)
            def _(p):
                for k in range(*groups_a[g]):
                    source = source_of(z, nz, k)
                    block = jnp.maximum(wsm[p, 0, source * rows + row_me], 0)
                    sa[p, k] = pairs[0, block] if k == 0 else ga[k - 1][block]

    def select_b(g):
        @pl.loop(0, cols)
        def _(p):
            for k in range(*groups_b[g]):
                source = source_of(y, ny, k)
                block = jnp.maximum(wsm[rows + p, 0, z * rows + source * CORES + c], 0)
                sb[p, k] = pairs[1, block] if k == 0 else gb[k - 1][block]

    def start_a(g):
        lo, hi = groups_a[g]
        part = pl.ds(lo, hi - lo)

        @pl.when(needed_a(g))
        def _():
            @pl.loop(1, rows)
            def _(d):
                send_a(d, g).start()

            pltpu.make_async_copy(
                sa.at[row_me, part], ra.at[row_me, part], a_recv.at[g, row_me]
            ).start()

    def start_b(g):
        lo, hi = groups_b[g]
        part = pl.ds(lo, hi - lo)

        @pl.loop(1, cols)
        def _(d):
            later, copy = send_b(d, g)

            @pl.when(later)
            def _():
                copy.start()

        pltpu.make_async_copy(
            sb.at[col_me, part], rb.at[col_me, part], b_recv.at[g, col_me]
        ).start()

    hops = {}
    last = max(nz, ny) // 2

    def ring_step(step):
        for axis, size in ((0, nz), (1, ny)):
            for way, count in ((0, size // 2), (1, (size - 1) // 2)):
                if 0 < step <= count:
                    hops[axis, way, step - 1].wait_recv()
                if step < count:
                    hops[axis, way, step] = ring_copy(axis, way, step)
                    hops[axis, way, step].start()

    ring_step(0)
    ring_step(1)
    pltpu.make_async_copy(wall, wall, want_recv).wait()
    to_smem = pltpu.make_async_copy(wall, wsm, smem_sem)
    to_smem.start()
    to_smem.wait()
    for step in range(1, last + 1):
        if step > 1:
            ring_step(step)
        now_a = [g for g, group in enumerate(groups_a) if sent_at(group) == step]
        now_b = [g for g, group in enumerate(groups_b) if sent_at(group) == step]
        for g in now_a:
            select_a(g)
        for g in now_b:
            select_b(g)
        for g in now_a:
            start_a(g)
        for g in now_b:
            start_b(g)

    loads[3].wait()
    product = jnp.dot(tokens[...], w_query[...], preferred_element_type=jnp.float32)
    for b in range(blocks):
        for h in range(0, heads, 2):
            wide = product[b * BLK : (b + 1) * BLK, h * HD : (h + 2) * HD]
            wide = turned(wide, b, False) * (HD ** -0.5)
            spot = pl.ds(b * BLK, BLK)
            query[h, spot] = jnp.where(value_side, 0.0, wide).astype(jnp.bfloat16)
            query[h + 1, spot] = jnp.where(
                value_side, 0.0, pltpu.roll(wide, HD, 1)
            ).astype(jnp.bfloat16)
    loads[4].wait()

    @pl.loop(0, rows)
    def _(p):
        for g, (lo, hi) in enumerate(groups_a):
            part = pl.ds(lo, hi - lo)

            @pl.when(needed_a(g))
            def _():
                pltpu.make_async_copy(sa.at[p, part], ra.at[p, part], a_recv.at[g, p]).wait()

    @pl.loop(0, cols)
    def _(p):
        @pl.when(p // CORES <= z)
        def _():
            for g, (lo, hi) in enumerate(groups_b):
                part = pl.ds(lo, hi - lo)
                pltpu.make_async_copy(sb.at[p, part], rb.at[p, part], b_recv.at[g, p]).wait()

    lag = 3
    out_rows = 2 * BLK
    key_lane = lax.broadcasted_iota(jnp.int32, (1, SEL * BLK), 1)
    query_row = lax.broadcasted_iota(jnp.int32, (BLK, SEL * BLK), 0)
    key_col = lax.broadcasted_iota(jnp.int32, (BLK, SEL * BLK), 1)
    causal = jnp.where((key_col < BLK) & (key_col > query_row), -jnp.inf, 0.0).astype(jnp.float32)

    def slot_of(place, size, owner):
        r = lax.rem(place - owner + size, size)
        return jnp.where(r <= size // 2, jnp.maximum(2 * r - 1, 0), 2 * (size - r))

    def attend_block(b):
        bias = jnp.zeros((1, SEL * BLK), jnp.float32)
        for s in range(SEL):
            named = chosen_ref[b, s]
            owner = lax.shift_right_arithmetic(named, 3)
            index = lax.bitwise_and(named, blocks - 1)
            here = (named < 0) | (owner == me)
            owner = jnp.where(here, me, owner)
            oz, oy, oc = owner // rows, lax.rem(owner, rows) // CORES, lax.rem(owner, CORES)
            kv[b, pl.ds(s * BLK, HALF)] = jnp.where(
                here, pairs[0, index], ra[oy * CORES + oc, slot_of(z, nz, oz)]
            )
            kv[b, pl.ds(s * BLK + HALF, HALF)] = jnp.where(
                here, pairs[1, index], rb[oz * CORES + oc, slot_of(y, ny, oy)]
            )
            if s > 0:
                bias = jnp.where((key_lane // BLK == s) & (named < 0), -jnp.inf, bias)
        keys = kv[b]
        queries = query[:, pl.ds(b * BLK, BLK), :].reshape(heads * BLK, 2 * HD)
        scores = lax.dot_general(
            queries, keys, (((1,), (1,)), ((), ())), preferred_element_type=jnp.float32
        )
        scores = scores.reshape(heads, BLK, SEL * BLK) + (causal + bias)[None]
        scores = scores.reshape(heads * BLK, SEL * BLK)
        peak = jnp.max(scores, axis=1, keepdims=True)
        weights = jnp.exp(scores - peak).astype(jnp.bfloat16)
        ones_or_values = jnp.where(value_side, keys, jnp.ones((), jnp.bfloat16))
        mixed = jnp.dot(weights, ones_or_values, preferred_element_type=jnp.float32)
        swapped = pltpu.roll(mixed, HD, 1)
        outs = []
        for h in range(0, heads, 2):
            lo = slice(h * BLK, (h + 1) * BLK)
            hi = slice((h + 1) * BLK, (h + 2) * BLK)
            outs.append(
                jnp.where(value_side, mixed[hi], swapped[lo])
                / jnp.where(value_side, swapped[hi], mixed[lo])
            )
        return jnp.concatenate(outs, axis=1).astype(jnp.bfloat16)

    def piece(owner, k):
        return full.at[owner, pl.ds(k * BLK, BLK)]

    def near(way, k):
        return pltpu.make_async_remote_copy(
            piece(t, k), piece(t, k), tp_send.at[way, k], tp_recv.at[way, k],
            device_id={"tp": (right, left)[way]}, device_id_type=MESH,
        )

    def onward(k):
        way = k % 2
        source = (left, right)[way]
        return pltpu.make_async_remote_copy(
            piece(source, k), piece(source, k), tp_send.at[2, k], tp_recv.at[2, k],
            device_id={"tp": (right, left)[way]}, device_id_type=MESH,
        )

    def pass_on(k):
        near(k % 2, k).wait_recv()
        onward(k).start()

    for b in range(blocks):
        full[t, pl.ds(b * BLK, BLK)] = attend_block(b)
        near(0, b).start()
        near(1, b).start()
        if b >= lag:
            pass_on(b - lag)
    for b in range(blocks - lag, blocks):
        pass_on(b)

    width = heads * HD
    for k in range(row_count // out_rows):
        for b in range(k * out_rows // BLK, (k + 1) * out_rows // BLK):
            near((b + 1) % 2, b).wait_recv()
            onward(b).wait_recv()
        total = None
        squares = None
        for owner in range(nt):
            wide = full[owner, pl.ds(k * out_rows, out_rows)].astype(jnp.float32)
            square = jnp.sum(wide * wide, axis=1, keepdims=True)
            scaled = (wide * gain_ref[:, pl.ds(owner * width, width)]).astype(jnp.bfloat16)
            term = jnp.dot(
                scaled,
                w_out[pl.ds(owner * width, width), :],
                preferred_element_type=jnp.float32,
            )
            total = term if total is None else total + term
            squares = square if squares is None else squares + square
        inverse = lax.rsqrt(squares / (HQ * HD) + norm_eps)
        out_ref[pl.ds(k * out_rows, out_rows), :] = (inverse * total).astype(jnp.bfloat16)

    for copy in hops.values():
        copy.wait_send()
    sends = wall.at[pl.ds(0, rows + cols - 2)]
    pltpu.make_async_copy(sends, sends, want_send).wait()

    @pl.loop(1, rows)
    def _(d):
        for g in range(len(groups_a)):
            @pl.when(needed_a(g))
            def _():
                send_a(d, g).wait_send()

    @pl.loop(1, cols)
    def _(d):
        for g in range(len(groups_b)):
            later, copy = send_b(d, g)

            @pl.when(later)
            def _():
                copy.wait_send()

    for k in range(blocks):
        near(0, k).wait_send()
        near(1, k).wait_send()
        onward(k).wait_send()


def per_device(tokens, w_query, w_key, w_value, w_out, out_gain, chosen):
    nz, ny, nt = lax.axis_size("kv_0"), lax.axis_size("kv_1"), lax.axis_size("tp")
    kv_place = lax.axis_index(KV)
    row_count, depth = tokens.shape
    blocks = row_count // BLK
    heads = w_query.shape[1] // HD
    rows, cols = ny * CORES, nz * CORES
    half_size = HD // 2
    frequency = rope_base ** (-jnp.arange(half_size, dtype=jnp.float32) / half_size)
    places = jnp.concatenate(
        [
            jnp.arange(BLK, dtype=jnp.int32),
            kv_place * row_count + BLK * jnp.arange(blocks, dtype=jnp.int32),
        ]
    )
    angles = places.astype(jnp.float32)[:, None] * jnp.tile(frequency, 4)[None, :]
    sign = jnp.where(jnp.arange(2 * HD) % HD < half_size, -1.0, 1.0)
    table = jnp.stack([jnp.cos(angles), jnp.sin(angles) * sign])

    piece = (HALF, 2 * HD)
    vmem = pl.BlockSpec(memory_space=pltpu.VMEM)
    far = pl.BlockSpec(memory_space=pltpu.HBM)
    dma = pltpu.SemaphoreType.DMA
    bf16 = jnp.bfloat16
    steps = max(nz, ny) // 2
    return pl.pallas_call(
        functools.partial(layer_kernel, nz, ny, nt),
        out_shape=jax.ShapeDtypeStruct((row_count, w_out.shape[1]), bf16),
        in_specs=[vmem, pl.BlockSpec(memory_space=pltpu.SMEM), vmem, vmem] + [far] * 5,
        out_specs=vmem,
        scratch_shapes=[
            pltpu.VMEM((row_count, depth), bf16),
            pltpu.VMEM((2 * HD, depth), bf16),
            pltpu.VMEM(w_query.shape, bf16),
            pltpu.VMEM(w_out.shape, bf16),
            pltpu.VMEM((2, blocks, *piece), bf16),
            pltpu.VMEM((heads, row_count, 2 * HD), bf16),
            [pltpu.VMEM((blocks, *piece), bf16)] * (nz - 1),
            [pltpu.VMEM((blocks, *piece), bf16)] * (ny - 1),
            pltpu.VMEM((rows, nz, *piece), bf16),
            pltpu.VMEM((cols, ny, *piece), bf16),
            pltpu.VMEM((rows, nz, *piece), bf16),
            pltpu.VMEM((cols, ny, *piece), bf16),
            pltpu.VMEM((1, 128), jnp.int32),
            pltpu.VMEM((rows + cols, 1, 128), jnp.int32),
            pltpu.SMEM((rows + cols, 1, 128), jnp.int32),
            pltpu.VMEM((blocks, SEL * BLK, 2 * HD), bf16),
            pltpu.VMEM((nt, row_count, heads * HD), bf16),
            dma((5,)),
            dma, dma, dma,
            dma((2, 2, steps)),
            dma((2, 2, steps)),
            dma((4, rows)),
            dma((4, rows)),
            dma((4, cols)),
            dma((4, cols)),
            dma((3, blocks)),
            dma((3, blocks)),
        ],
        compiler_params=pltpu.CompilerParams(collective_id=0, has_side_effects=True),
    )(
        chosen[0], chosen[0], table, out_gain[None, :],
        tokens, w_key.T, w_value.T, w_query, w_out,
    )


def solution(mesh):
    count = mesh.shape["kv"]
    ny = 8 if count == 128 else 2
    nz = count // (ny * CORES)
    finer = Mesh(
        mesh.devices.reshape(nz, ny, CORES, mesh.shape["tp"]), ("kv_0", "kv_1", "kv_2", "tp")
    )
    placed = (
        P(KV, None),
        P(None, "tp"),
        P(None, "tp"),
        P(None, "tp"),
        P(None, "tp"),
        P(),
        P("tp", KV, None),
    )
    return jax.shard_map(
        per_device, mesh=finer, in_specs=placed, out_specs=P(KV, "tp"), check_vma=False
    )
```

```python
import functools

import jax
import jax.numpy as jnp
import numpy as np
from jax import lax
from jax.experimental import pallas as pl
from jax.experimental.pallas import tpu as pltpu
from jax.sharding import Mesh
from jax.sharding import PartitionSpec as P

HQ = 16
HD = 64
BLK = 64
SEL = 8
HALF = BLK // 2
CORES = 2
KV = ("kv_0", "kv_1", "kv_2")
MESH = pl.DeviceIdType.MESH

rope_base = 500000.0
norm_eps = 1e-06


def layer_kernel(
    nz, ny, nt,
    chosen_hbm, gain_hbm, frequency_hbm, tokens_hbm, wk_hbm, wv_hbm, wq_hbm, wo_hbm, out_ref,
    ids_ref, chosen_ref, gain_ref, frequency_ref, cos_ref, sin_ref,
    tokens, w_pair, w_query, w_out, pairs, query, ga, gb, sa, sb, ra, rb, want, wall, wsm, kv, full,
    load_sem, want_send, want_recv, smem_sem, ring_send, ring_recv,
    a_send, a_recv, b_send, b_recv, tp_send, tp_recv,
):
    z, y, c = lax.axis_index("kv_0"), lax.axis_index("kv_1"), lax.axis_index("kv_2")
    t = lax.axis_index("tp")
    rows, cols = ny * CORES, nz * CORES
    row_me, col_me = y * CORES + c, z * CORES + c
    blocks = pairs.shape[1]
    me = z * rows + row_me
    heads, row_count = query.shape[0], query.shape[1]

    def row_peer(d):
        p = lax.rem(row_me + d, rows)
        return p, {"kv_0": z, "kv_1": p // CORES, "kv_2": lax.rem(p, CORES)}

    def col_peer(d):
        p = lax.rem(col_me + d, cols)
        return p, {"kv_0": p // CORES, "kv_1": y, "kv_2": lax.rem(p, CORES)}

    right, left = lax.rem(t + 1, nt), lax.rem(t + nt - 1, nt)
    barrier = pltpu.get_barrier_semaphore()

    @pl.loop(1, rows)
    def _(d):
        _, peer = row_peer(d)
        pl.semaphore_signal(barrier, inc=1, device_id=peer, device_id_type=MESH)

    @pl.loop(1, nz)
    def _(d):
        for core in range(CORES):
            peer = {"kv_0": lax.rem(z + d, nz), "kv_1": y, "kv_2": core}
            pl.semaphore_signal(barrier, inc=1, device_id=peer, device_id_type=MESH)

    for peer in (right, left):
        pl.semaphore_signal(barrier, inc=1, device_id={"tp": peer}, device_id_type=MESH)

    loads = [
        pltpu.make_async_copy(source, target, load_sem.at[k])
        for k, (source, target) in enumerate(
            (
                (chosen_hbm, ids_ref),
                (frequency_hbm, frequency_ref),
                (wk_hbm, w_pair.at[pl.ds(0, HD)]),
                (wv_hbm, w_pair.at[pl.ds(HD, HD)]),
                (tokens_hbm, tokens),
                (wq_hbm, w_query),
                (wo_hbm, w_out),
                (gain_hbm, gain_ref),
                (chosen_hbm, chosen_ref),
            )
        )
    ]
    for load in loads:
        load.start()

    head_lane = lax.broadcasted_iota(jnp.int32, (1, 2 * HD), 1)
    value_side = head_lane >= HD
    lower_side = head_lane % HD < HD // 2
    loads[0].wait()
    loads[1].wait()
    place = lax.broadcasted_iota(jnp.int32, (BLK + blocks, 2 * HD), 0)
    place = jnp.where(place < BLK, place, (me * blocks + place - BLK) * BLK)
    angles = place.astype(jnp.float32) * frequency_ref[...]
    cos_ref[...] = jnp.cos(angles)
    sin_ref[...] = jnp.sin(angles) * jnp.where(lower_side, -1.0, 1.0)

    lane = lax.broadcasted_iota(jnp.int32, (blocks, 128), 1)
    found = jnp.full((blocks, 128), -1, jnp.int32)
    for s in range(SEL):
        ids = jnp.broadcast_to(ids_ref[:, s : s + 1], (blocks, 128))
        hit = (ids // blocks == lane) & (ids >= 0) & (lane != me)
        found = jnp.maximum(found, jnp.where(hit, ids % blocks, -1))
    want[...] = jnp.max(found, axis=0, keepdims=True)

    def turned(wide, b, only_keys):
        cos_row, sin_row = cos_ref[pl.ds(0, BLK)], sin_ref[pl.ds(0, BLK)]
        cos_base, sin_base = cos_ref[pl.ds(BLK + b, 1)], sin_ref[pl.ds(BLK + b, 1)]
        cosine = cos_base * cos_row - sin_base * sin_row
        sine_wave = sin_base * cos_row + cos_base * sin_row
        if only_keys:
            cosine = jnp.where(value_side, 1.0, cosine)
            sine_wave = jnp.where(value_side, 0.0, sine_wave)
        other = jnp.where(lower_side, pltpu.roll(wide, 3 * HD // 2, 1), pltpu.roll(wide, HD // 2, 1))
        return wide * cosine + other * sine_wave

    for load in loads[2:5]:
        load.wait()
    pair = lax.dot_general(
        tokens[...], w_pair[...], (((1,), (1,)), ((), ())), preferred_element_type=jnp.float32
    )
    for b in range(blocks):
        held = turned(pair[b * BLK : (b + 1) * BLK], b, True).astype(jnp.bfloat16)
        pairs[0, b] = held[:HALF]
        pairs[1, b] = held[HALF:]

    pl.semaphore_wait(barrier, rows - 1 + (nz - 1) * CORES + 2)

    pltpu.make_async_copy(want, wall.at[row_me], want_recv).start()
    pltpu.make_async_copy(want, wall.at[rows + col_me], want_recv).start()

    @pl.loop(1, rows)
    def _(d):
        _, peer = row_peer(d)
        pltpu.make_async_remote_copy(
            want, wall.at[row_me], want_send, want_recv, device_id=peer, device_id_type=MESH
        ).start()

    @pl.loop(1, cols)
    def _(d):
        _, peer = col_peer(d)
        pltpu.make_async_remote_copy(
            want, wall.at[rows + col_me], want_send, want_recv, device_id=peer, device_id_type=MESH
        ).start()

    def ring_copy(axis, way, step):
        name, place, size, held = (("kv_0", z, nz, ga), ("kv_1", y, ny, gb))[axis]
        target = lax.rem(place + (1, size - 1)[way], size)
        return pltpu.make_async_remote_copy(
            pairs.at[axis] if step == 0 else held[2 * step - 2 + way],
            held[2 * step + way],
            ring_send.at[axis, way, step],
            ring_recv.at[axis, way, step],
            device_id={name: target},
            device_id_type=MESH,
        )

    def source_of(place, size, k):
        if k % 2:
            return lax.rem(place - (k + 1) // 2 + size, size)
        return lax.rem(place + k // 2, size)

    def groups_of(size):
        found = [(0, 1)]
        for s in range(1, size // 2 + 1):
            found.append((2 * s - 1, min(2 * s + 1, size)))
        if size >= 8:
            found[-2:] = [(found[-2][0], found[-1][1])]
        return found

    def sent_at(group):
        return min(group[1] // 2 + 1, last)

    groups_a, groups_b = groups_of(nz), groups_of(ny)

    def send_a(d, g):
        p, peer = row_peer(d)
        lo, hi = groups_a[g]
        part = pl.ds(lo, hi - lo)
        return pltpu.make_async_remote_copy(
            sa.at[p, part], ra.at[row_me, part], a_send.at[g, p], a_recv.at[g, row_me],
            device_id=peer, device_id_type=MESH,
        )

    def send_b(d, g):
        p, peer = col_peer(d)
        lo, hi = groups_b[g]
        part = pl.ds(lo, hi - lo)
        copy = pltpu.make_async_remote_copy(
            sb.at[p, part], rb.at[col_me, part], b_send.at[g, p], b_recv.at[g, col_me],
            device_id=peer, device_id_type=MESH,
        )
        return p // CORES >= z, copy

    def needed_a(g):
        return z >= (groups_a[g][0] + 1) // 2

    def select_a(g):
        @pl.when(needed_a(g))
        def _():
            @pl.loop(0, rows)
            def _(p):
                for k in range(*groups_a[g]):
                    source = source_of(z, nz, k)
                    block = jnp.maximum(wsm[p, 0, source * rows + row_me], 0)
                    sa[p, k] = pairs[0, block] if k == 0 else ga[k - 1][block]

    def select_b(g):
        @pl.loop(0, cols)
        def _(p):
            for k in range(*groups_b[g]):
                source = source_of(y, ny, k)
                block = jnp.maximum(wsm[rows + p, 0, z * rows + source * CORES + c], 0)
                sb[p, k] = pairs[1, block] if k == 0 else gb[k - 1][block]

    def start_a(g):
        lo, hi = groups_a[g]
        part = pl.ds(lo, hi - lo)

        @pl.when(needed_a(g))
        def _():
            @pl.loop(1, rows)
            def _(d):
                send_a(d, g).start()

            pltpu.make_async_copy(
                sa.at[row_me, part], ra.at[row_me, part], a_recv.at[g, row_me]
            ).start()

    def start_b(g):
        lo, hi = groups_b[g]
        part = pl.ds(lo, hi - lo)

        @pl.loop(1, cols)
        def _(d):
            later, copy = send_b(d, g)

            @pl.when(later)
            def _():
                copy.start()

        pltpu.make_async_copy(
            sb.at[col_me, part], rb.at[col_me, part], b_recv.at[g, col_me]
        ).start()

    hops = {}
    last = max(nz, ny) // 2

    def ring_step(step):
        for axis, size in ((0, nz), (1, ny)):
            for way, count in ((0, size // 2), (1, (size - 1) // 2)):
                if 0 < step <= count:
                    hops[axis, way, step - 1].wait_recv()
                if step < count:
                    hops[axis, way, step] = ring_copy(axis, way, step)
                    hops[axis, way, step].start()

    ring_step(0)
    ring_step(1)
    pltpu.make_async_copy(wall, wall, want_recv).wait()
    to_smem = pltpu.make_async_copy(wall, wsm, smem_sem)
    to_smem.start()
    to_smem.wait()
    for step in range(1, last + 1):
        if step > 1:
            ring_step(step)
        now_a = [g for g, group in enumerate(groups_a) if sent_at(group) == step]
        now_b = [g for g, group in enumerate(groups_b) if sent_at(group) == step]
        for g in now_a:
            select_a(g)
        for g in now_b:
            select_b(g)
        for g in now_a:
            start_a(g)
        for g in now_b:
            start_b(g)

    loads[5].wait()
    product = jnp.dot(tokens[...], w_query[...], preferred_element_type=jnp.float32)
    for b in range(blocks):
        for h in range(0, heads, 2):
            wide = product[b * BLK : (b + 1) * BLK, h * HD : (h + 2) * HD]
            wide = turned(wide, b, False) * (HD ** -0.5)
            spot = pl.ds(b * BLK, BLK)
            query[h, spot] = jnp.where(value_side, 0.0, wide).astype(jnp.bfloat16)
            query[h + 1, spot] = jnp.where(
                value_side, 0.0, pltpu.roll(wide, HD, 1)
            ).astype(jnp.bfloat16)
    for load in loads[6:]:
        load.wait()

    @pl.loop(0, rows)
    def _(p):
        for g, (lo, hi) in enumerate(groups_a):
            part = pl.ds(lo, hi - lo)

            @pl.when(needed_a(g))
            def _():
                pltpu.make_async_copy(sa.at[p, part], ra.at[p, part], a_recv.at[g, p]).wait()

    @pl.loop(0, cols)
    def _(p):
        @pl.when(p // CORES <= z)
        def _():
            for g, (lo, hi) in enumerate(groups_b):
                part = pl.ds(lo, hi - lo)
                pltpu.make_async_copy(sb.at[p, part], rb.at[p, part], b_recv.at[g, p]).wait()

    lag = 3
    out_rows = 2 * BLK
    key_lane = lax.broadcasted_iota(jnp.int32, (1, SEL * BLK), 1)
    query_row = lax.broadcasted_iota(jnp.int32, (BLK, SEL * BLK), 0)
    key_col = lax.broadcasted_iota(jnp.int32, (BLK, SEL * BLK), 1)
    causal = jnp.where((key_col < BLK) & (key_col > query_row), -jnp.inf, 0.0).astype(jnp.float32)

    def slot_of(place, size, owner):
        r = lax.rem(place - owner + size, size)
        return jnp.where(r <= size // 2, jnp.maximum(2 * r - 1, 0), 2 * (size - r))

    def attend_block(b):
        bias = jnp.zeros((1, SEL * BLK), jnp.float32)
        for s in range(SEL):
            named = chosen_ref[b, s]
            owner = lax.shift_right_arithmetic(named, 3)
            index = lax.bitwise_and(named, blocks - 1)
            here = (named < 0) | (owner == me)
            owner = jnp.where(here, me, owner)
            oz, oy, oc = owner // rows, lax.rem(owner, rows) // CORES, lax.rem(owner, CORES)
            kv[b, pl.ds(s * BLK, HALF)] = jnp.where(
                here, pairs[0, index], ra[oy * CORES + oc, slot_of(z, nz, oz)]
            )
            kv[b, pl.ds(s * BLK + HALF, HALF)] = jnp.where(
                here, pairs[1, index], rb[oz * CORES + oc, slot_of(y, ny, oy)]
            )
            if s > 0:
                bias = jnp.where((key_lane // BLK == s) & (named < 0), -jnp.inf, bias)
        keys = kv[b]
        queries = query[:, pl.ds(b * BLK, BLK), :].reshape(heads * BLK, 2 * HD)
        scores = lax.dot_general(
            queries, keys, (((1,), (1,)), ((), ())), preferred_element_type=jnp.float32
        )
        scores = scores.reshape(heads, BLK, SEL * BLK) + (causal + bias)[None]
        scores = scores.reshape(heads * BLK, SEL * BLK)
        peak = jnp.max(scores, axis=1, keepdims=True)
        weights = jnp.exp(scores - peak).astype(jnp.bfloat16)
        ones_or_values = jnp.where(value_side, keys, jnp.ones((), jnp.bfloat16))
        mixed = jnp.dot(weights, ones_or_values, preferred_element_type=jnp.float32)
        swapped = pltpu.roll(mixed, HD, 1)
        outs = []
        for h in range(0, heads, 2):
            lo = slice(h * BLK, (h + 1) * BLK)
            hi = slice((h + 1) * BLK, (h + 2) * BLK)
            outs.append(
                jnp.where(value_side, mixed[hi], swapped[lo])
                / jnp.where(value_side, swapped[hi], mixed[lo])
            )
        return jnp.concatenate(outs, axis=1).astype(jnp.bfloat16)

    def piece(owner, k):
        return full.at[owner, pl.ds(k * BLK, BLK)]

    def near(way, k):
        return pltpu.make_async_remote_copy(
            piece(t, k), piece(t, k), tp_send.at[way, k], tp_recv.at[way, k],
            device_id={"tp": (right, left)[way]}, device_id_type=MESH,
        )

    def onward(k):
        way = k % 2
        source = (left, right)[way]
        return pltpu.make_async_remote_copy(
            piece(source, k), piece(source, k), tp_send.at[2, k], tp_recv.at[2, k],
            device_id={"tp": (right, left)[way]}, device_id_type=MESH,
        )

    def pass_on(k):
        near(k % 2, k).wait_recv()
        onward(k).start()

    for b in range(blocks):
        full[t, pl.ds(b * BLK, BLK)] = attend_block(b)
        near(0, b).start()
        near(1, b).start()
        if b >= lag:
            pass_on(b - lag)
    for b in range(blocks - lag, blocks):
        pass_on(b)

    width = heads * HD
    for k in range(row_count // out_rows):
        for b in range(k * out_rows // BLK, (k + 1) * out_rows // BLK):
            near((b + 1) % 2, b).wait_recv()
            onward(b).wait_recv()
        total = None
        squares = None
        for owner in range(nt):
            wide = full[owner, pl.ds(k * out_rows, out_rows)].astype(jnp.float32)
            square = jnp.sum(wide * wide, axis=1, keepdims=True)
            scaled = (wide * gain_ref[:, pl.ds(owner * width, width)]).astype(jnp.bfloat16)
            term = jnp.dot(
                scaled,
                w_out[pl.ds(owner * width, width), :],
                preferred_element_type=jnp.float32,
            )
            total = term if total is None else total + term
            squares = square if squares is None else squares + square
        inverse = lax.rsqrt(squares / (HQ * HD) + norm_eps)
        out_ref[pl.ds(k * out_rows, out_rows), :] = (inverse * total).astype(jnp.bfloat16)

    for copy in hops.values():
        copy.wait_send()
    sends = wall.at[pl.ds(0, rows + cols - 2)]
    pltpu.make_async_copy(sends, sends, want_send).wait()

    @pl.loop(1, rows)
    def _(d):
        for g in range(len(groups_a)):
            @pl.when(needed_a(g))
            def _():
                send_a(d, g).wait_send()

    @pl.loop(1, cols)
    def _(d):
        for g in range(len(groups_b)):
            later, copy = send_b(d, g)

            @pl.when(later)
            def _():
                copy.wait_send()

    for k in range(blocks):
        near(0, k).wait_send()
        near(1, k).wait_send()
        onward(k).wait_send()


def per_device(tokens, w_query, w_key, w_value, w_out, out_gain, chosen):
    nz, ny, nt = lax.axis_size("kv_0"), lax.axis_size("kv_1"), lax.axis_size("tp")
    row_count, depth = tokens.shape
    blocks = row_count // BLK
    heads = w_query.shape[1] // HD
    rows, cols = ny * CORES, nz * CORES
    half_size = HD // 2
    frequency = np.float64(rope_base) ** (-np.arange(half_size) / half_size)
    frequency = jnp.asarray(np.tile(frequency, 4)[None, :], jnp.float32)

    piece = (HALF, 2 * HD)
    vmem = pl.BlockSpec(memory_space=pltpu.VMEM)
    far = pl.BlockSpec(memory_space=pltpu.HBM)
    dma = pltpu.SemaphoreType.DMA
    bf16 = jnp.bfloat16
    steps = max(nz, ny) // 2
    return pl.pallas_call(
        functools.partial(layer_kernel, nz, ny, nt),
        out_shape=jax.ShapeDtypeStruct((row_count, w_out.shape[1]), bf16),
        in_specs=[far] * 8,
        out_specs=vmem,
        scratch_shapes=[
            pltpu.VMEM(chosen.shape[1:], jnp.int32),
            pltpu.SMEM(chosen.shape[1:], jnp.int32),
            pltpu.VMEM((1, out_gain.shape[0]), jnp.float32),
            pltpu.VMEM((1, 2 * HD), jnp.float32),
            pltpu.VMEM((BLK + blocks, 2 * HD), jnp.float32),
            pltpu.VMEM((BLK + blocks, 2 * HD), jnp.float32),
            pltpu.VMEM((row_count, depth), bf16),
            pltpu.VMEM((2 * HD, depth), bf16),
            pltpu.VMEM(w_query.shape, bf16),
            pltpu.VMEM(w_out.shape, bf16),
            pltpu.VMEM((2, blocks, *piece), bf16),
            pltpu.VMEM((heads, row_count, 2 * HD), bf16),
            [pltpu.VMEM((blocks, *piece), bf16)] * (nz - 1),
            [pltpu.VMEM((blocks, *piece), bf16)] * (ny - 1),
            pltpu.VMEM((rows, nz, *piece), bf16),
            pltpu.VMEM((cols, ny, *piece), bf16),
            pltpu.VMEM((rows, nz, *piece), bf16),
            pltpu.VMEM((cols, ny, *piece), bf16),
            pltpu.VMEM((1, 128), jnp.int32),
            pltpu.VMEM((rows + cols, 1, 128), jnp.int32),
            pltpu.SMEM((rows + cols, 1, 128), jnp.int32),
            pltpu.VMEM((blocks, SEL * BLK, 2 * HD), bf16),
            pltpu.VMEM((nt, row_count, heads * HD), bf16),
            dma((9,)),
            dma, dma, dma,
            dma((2, 2, steps)),
            dma((2, 2, steps)),
            dma((4, rows)),
            dma((4, rows)),
            dma((4, cols)),
            dma((4, cols)),
            dma((3, blocks)),
            dma((3, blocks)),
        ],
        compiler_params=pltpu.CompilerParams(collective_id=0, has_side_effects=True, vmem_limit_bytes=40*2**20),
    )(
        *(
            pltpu.with_memory_space_constraint(a, pltpu.HBM)
            for a in (
                chosen[0], out_gain[None, :], frequency,
                tokens, w_key.T, w_value.T, w_query, w_out,
            )
        )
    )


def solution(mesh):
    count = mesh.shape["kv"]
    ny = 8 if count == 128 else 2
    nz = count // (ny * CORES)
    finer = Mesh(
        mesh.devices.reshape(nz, ny, CORES, mesh.shape["tp"]), ("kv_0", "kv_1", "kv_2", "tp")
    )
    placed = (
        P(KV, None),
        P(None, "tp"),
        P(None, "tp"),
        P(None, "tp"),
        P(None, "tp"),
        P(),
        P("tp", KV, None),
    )
    return jax.shard_map(
        per_device, mesh=finer, in_specs=placed, out_specs=P(KV, "tp"), check_vma=False
    )
```

```python
import functools

import jax
import jax.numpy as jnp
import numpy as np
from jax import lax
from jax.experimental import pallas as pl
from jax.experimental.pallas import tpu as pltpu
from jax.sharding import Mesh
from jax.sharding import PartitionSpec as P

HQ = 16
HD = 64
BLK = 64
SEL = 8
HALF = BLK // 2
CORES = 2
KV = ("kv_0", "kv_1", "kv_2")
MESH = pl.DeviceIdType.MESH

rope_base = 500000.0
norm_eps = 1e-06


def layer_kernel(
    nz, ny, nt,
    chosen_hbm, gain_hbm, frequency_hbm, tokens_hbm, wk_hbm, wv_hbm, wq_hbm, wo_hbm, out_ref,
    ids_ref, chosen_ref, gain_ref, frequency_ref, cos_ref, sin_ref,
    tokens, w_pair, w_query, w_out, pairs, query, ga, gb, sa, sb, ra, rb, want, wall, wsm, kv, full,
    load_sem, want_send, want_recv, smem_sem, ring_send, ring_recv,
    a_send, a_recv, b_send, b_recv, tp_send, tp_recv,
):
    z, y, c = lax.axis_index("kv_0"), lax.axis_index("kv_1"), lax.axis_index("kv_2")
    t = lax.axis_index("tp")
    rows, cols = ny * CORES, nz * CORES
    row_me, col_me = y * CORES + c, z * CORES + c
    blocks = pairs.shape[1]
    me = z * rows + row_me
    heads, row_count = query.shape[0], query.shape[1]

    def row_peer(d):
        p = lax.rem(row_me + d, rows)
        return p, {"kv_0": z, "kv_1": p // CORES, "kv_2": lax.rem(p, CORES)}

    def col_peer(d):
        p = lax.rem(col_me + d, cols)
        return p, {"kv_0": p // CORES, "kv_1": y, "kv_2": lax.rem(p, CORES)}

    right, left = lax.rem(t + 1, nt), lax.rem(t + nt - 1, nt)
    barrier = pltpu.get_barrier_semaphore()

    @pl.loop(1, rows)
    def _(d):
        _, peer = row_peer(d)
        pl.semaphore_signal(barrier, inc=1, device_id=peer, device_id_type=MESH)

    @pl.loop(1, nz)
    def _(d):
        for core in range(CORES):
            peer = {"kv_0": lax.rem(z + d, nz), "kv_1": y, "kv_2": core}
            pl.semaphore_signal(barrier, inc=1, device_id=peer, device_id_type=MESH)

    for peer in (right, left):
        pl.semaphore_signal(barrier, inc=1, device_id={"tp": peer}, device_id_type=MESH)

    loads = [
        pltpu.make_async_copy(source, target, load_sem.at[k])
        for k, (source, target) in enumerate(
            (
                (chosen_hbm, ids_ref),
                (frequency_hbm, frequency_ref),
                (wk_hbm, w_pair.at[pl.ds(0, HD)]),
                (wv_hbm, w_pair.at[pl.ds(HD, HD)]),
                (tokens_hbm, tokens),
                (wq_hbm, w_query),
                (wo_hbm, w_out),
                (gain_hbm, gain_ref),
                (chosen_hbm, chosen_ref),
            )
        )
    ]
    for load in loads:
        load.start()

    head_lane = lax.broadcasted_iota(jnp.int32, (1, 2 * HD), 1)
    value_side = head_lane >= HD
    lower_side = head_lane % HD < HD // 2
    loads[0].wait()
    loads[1].wait()
    place = lax.broadcasted_iota(jnp.int32, (BLK + blocks, 2 * HD), 0)
    place = jnp.where(place < BLK, place, (me * blocks + place - BLK) * BLK)
    angles = place.astype(jnp.float32) * frequency_ref[...]
    cos_ref[...] = jnp.cos(angles)
    sin_ref[...] = jnp.sin(angles) * jnp.where(lower_side, -1.0, 1.0)

    lane = lax.broadcasted_iota(jnp.int32, (blocks, 128), 1)
    found = jnp.full((blocks, 128), -1, jnp.int32)
    for s in range(SEL):
        ids = jnp.broadcast_to(ids_ref[:, s : s + 1], (blocks, 128))
        hit = (ids // blocks == lane) & (ids >= 0) & (lane != me)
        found = jnp.maximum(found, jnp.where(hit, ids % blocks, -1))
    want[...] = jnp.max(found, axis=0, keepdims=True)

    def turned(wide, b, only_keys):
        cos_row, sin_row = cos_ref[pl.ds(0, BLK)], sin_ref[pl.ds(0, BLK)]
        cos_base, sin_base = cos_ref[pl.ds(BLK + b, 1)], sin_ref[pl.ds(BLK + b, 1)]
        cosine = cos_base * cos_row - sin_base * sin_row
        sine_wave = sin_base * cos_row + cos_base * sin_row
        if only_keys:
            cosine = jnp.where(value_side, 1.0, cosine)
            sine_wave = jnp.where(value_side, 0.0, sine_wave)
        other = jnp.where(lower_side, pltpu.roll(wide, 3 * HD // 2, 1), pltpu.roll(wide, HD // 2, 1))
        return wide * cosine + other * sine_wave

    for load in loads[2:5]:
        load.wait()
    pair = lax.dot_general(
        tokens[...], w_pair[...], (((1,), (1,)), ((), ())), preferred_element_type=jnp.float32
    )
    for b in range(blocks):
        held = turned(pair[b * BLK : (b + 1) * BLK], b, True).astype(jnp.bfloat16)
        pairs[0, b] = held[:HALF]
        pairs[1, b] = held[HALF:]

    pl.semaphore_wait(barrier, rows - 1 + (nz - 1) * CORES + 2)

    pltpu.make_async_copy(want, wall.at[row_me], want_recv).start()
    pltpu.make_async_copy(want, wall.at[rows + col_me], want_recv).start()

    @pl.loop(1, rows)
    def _(d):
        _, peer = row_peer(d)
        pltpu.make_async_remote_copy(
            want, wall.at[row_me], want_send, want_recv, device_id=peer, device_id_type=MESH
        ).start()

    @pl.loop(1, cols)
    def _(d):
        _, peer = col_peer(d)
        pltpu.make_async_remote_copy(
            want, wall.at[rows + col_me], want_send, want_recv, device_id=peer, device_id_type=MESH
        ).start()

    def ring_copy(axis, way, step):
        name, place, size, held = (("kv_0", z, nz, ga), ("kv_1", y, ny, gb))[axis]
        target = lax.rem(place + (1, size - 1)[way], size)
        return pltpu.make_async_remote_copy(
            pairs.at[axis] if step == 0 else held[2 * step - 2 + way],
            held[2 * step + way],
            ring_send.at[axis, way, step],
            ring_recv.at[axis, way, step],
            device_id={name: target},
            device_id_type=MESH,
        )

    def source_of(place, size, k):
        if k % 2:
            return lax.rem(place - (k + 1) // 2 + size, size)
        return lax.rem(place + k // 2, size)

    def groups_of(size):
        found = [(0, 1)]
        for s in range(1, size // 2 + 1):
            found.append((2 * s - 1, min(2 * s + 1, size)))
        if size >= 8:
            found[-2:] = [(found[-2][0], found[-1][1])]
        return found

    def sent_at(group):
        return min(group[1] // 2 + 1, last)

    groups_a, groups_b = groups_of(nz), groups_of(ny)

    def send_a(d, g):
        p, peer = row_peer(d)
        lo, hi = groups_a[g]
        part = pl.ds(lo, hi - lo)
        return pltpu.make_async_remote_copy(
            sa.at[p, part], ra.at[row_me, part], a_send.at[g, p], a_recv.at[g, row_me],
            device_id=peer, device_id_type=MESH,
        )

    def send_b(d, g):
        p, peer = col_peer(d)
        lo, hi = groups_b[g]
        part = pl.ds(lo, hi - lo)
        copy = pltpu.make_async_remote_copy(
            sb.at[p, part], rb.at[col_me, part], b_send.at[g, p], b_recv.at[g, col_me],
            device_id=peer, device_id_type=MESH,
        )
        return p // CORES >= z, copy

    def needed_a(g):
        return z >= (groups_a[g][0] + 1) // 2

    def select_a(g):
        @pl.when(needed_a(g))
        def _():
            @pl.loop(0, rows)
            def _(p):
                for k in range(*groups_a[g]):
                    source = source_of(z, nz, k)
                    block = jnp.maximum(wsm[p, 0, source * rows + row_me], 0)
                    sa[p, k] = pairs[0, block] if k == 0 else ga[k - 1][block]

    def select_b(g):
        @pl.loop(0, cols)
        def _(p):
            for k in range(*groups_b[g]):
                source = source_of(y, ny, k)
                block = jnp.maximum(wsm[rows + p, 0, z * rows + source * CORES + c], 0)
                sb[p, k] = pairs[1, block] if k == 0 else gb[k - 1][block]

    def start_a(g):
        lo, hi = groups_a[g]
        part = pl.ds(lo, hi - lo)

        @pl.when(needed_a(g))
        def _():
            @pl.loop(1, rows)
            def _(d):
                send_a(d, g).start()

            pltpu.make_async_copy(
                sa.at[row_me, part], ra.at[row_me, part], a_recv.at[g, row_me]
            ).start()

    def start_b(g):
        lo, hi = groups_b[g]
        part = pl.ds(lo, hi - lo)

        @pl.loop(1, cols)
        def _(d):
            later, copy = send_b(d, g)

            @pl.when(later)
            def _():
                copy.start()

        pltpu.make_async_copy(
            sb.at[col_me, part], rb.at[col_me, part], b_recv.at[g, col_me]
        ).start()

    hops = {}
    last = max(nz, ny) // 2

    def ring_step(step):
        for axis, size in ((0, nz), (1, ny)):
            for way, count in ((0, size // 2), (1, (size - 1) // 2)):
                if 0 < step <= count:
                    hops[axis, way, step - 1].wait_recv()
                if step < count:
                    hops[axis, way, step] = ring_copy(axis, way, step)
                    hops[axis, way, step].start()

    ring_step(0)
    ring_step(1)
    pltpu.make_async_copy(wall, wall, want_recv).wait()
    to_smem = pltpu.make_async_copy(wall, wsm, smem_sem)
    to_smem.start()
    to_smem.wait()
    for step in range(1, last + 1):
        if step > 1:
            ring_step(step)
        now_a = [g for g, group in enumerate(groups_a) if sent_at(group) == step]
        now_b = [g for g, group in enumerate(groups_b) if sent_at(group) == step]
        for g in now_a:
            select_a(g)
        for g in now_b:
            select_b(g)
        for g in now_a:
            start_a(g)
        for g in now_b:
            start_b(g)

    loads[5].wait()
    product = jnp.dot(tokens[...], w_query[...], preferred_element_type=jnp.float32)
    for b in range(blocks):
        for h in range(0, heads, 2):
            wide = product[b * BLK : (b + 1) * BLK, h * HD : (h + 2) * HD]
            wide = turned(wide, b, False) * (HD ** -0.5)
            spot = pl.ds(b * BLK, BLK)
            query[h, spot] = jnp.where(value_side, 0.0, wide).astype(jnp.bfloat16)
            query[h + 1, spot] = jnp.where(
                value_side, 0.0, pltpu.roll(wide, HD, 1)
            ).astype(jnp.bfloat16)
    for load in loads[6:]:
        load.wait()

    @pl.loop(0, rows)
    def _(p):
        for g, (lo, hi) in enumerate(groups_a):
            part = pl.ds(lo, hi - lo)

            @pl.when(needed_a(g))
            def _():
                pltpu.make_async_copy(sa.at[p, part], ra.at[p, part], a_recv.at[g, p]).wait()

    @pl.loop(0, cols)
    def _(p):
        @pl.when(p // CORES <= z)
        def _():
            for g, (lo, hi) in enumerate(groups_b):
                part = pl.ds(lo, hi - lo)
                pltpu.make_async_copy(sb.at[p, part], rb.at[p, part], b_recv.at[g, p]).wait()

    out_rows = 2 * BLK
    key_lane = lax.broadcasted_iota(jnp.int32, (1, SEL * BLK), 1)
    query_row = lax.broadcasted_iota(jnp.int32, (BLK, SEL * BLK), 0)
    key_col = lax.broadcasted_iota(jnp.int32, (BLK, SEL * BLK), 1)
    causal = jnp.where((key_col < BLK) & (key_col > query_row), -jnp.inf, 0.0).astype(jnp.float32)

    def slot_of(place, size, owner):
        r = lax.rem(place - owner + size, size)
        return jnp.where(r <= size // 2, jnp.maximum(2 * r - 1, 0), 2 * (size - r))

    def attend_block(b):
        bias = jnp.zeros((1, SEL * BLK), jnp.float32)
        for s in range(SEL):
            named = chosen_ref[b, s]
            owner = lax.shift_right_arithmetic(named, 3)
            index = lax.bitwise_and(named, blocks - 1)
            here = (named < 0) | (owner == me)
            owner = jnp.where(here, me, owner)
            oz, oy, oc = owner // rows, lax.rem(owner, rows) // CORES, lax.rem(owner, CORES)
            kv[b, pl.ds(s * BLK, HALF)] = jnp.where(
                here, pairs[0, index], ra[oy * CORES + oc, slot_of(z, nz, oz)]
            )
            kv[b, pl.ds(s * BLK + HALF, HALF)] = jnp.where(
                here, pairs[1, index], rb[oz * CORES + oc, slot_of(y, ny, oy)]
            )
            if s > 0:
                bias = jnp.where((key_lane // BLK == s) & (named < 0), -jnp.inf, bias)
        keys = kv[b]
        queries = query[:, pl.ds(b * BLK, BLK), :].reshape(heads * BLK, 2 * HD)
        scores = lax.dot_general(
            queries, keys, (((1,), (1,)), ((), ())), preferred_element_type=jnp.float32
        )
        scores = scores.reshape(heads, BLK, SEL * BLK) + (causal + bias)[None]
        scores = scores.reshape(heads * BLK, SEL * BLK)
        peak = jnp.max(scores, axis=1, keepdims=True)
        weights = jnp.exp(scores - peak).astype(jnp.bfloat16)
        ones_or_values = jnp.where(value_side, keys, jnp.ones((), jnp.bfloat16))
        mixed = jnp.dot(weights, ones_or_values, preferred_element_type=jnp.float32)
        swapped = pltpu.roll(mixed, HD, 1)
        outs = []
        for h in range(0, heads, 2):
            lo = slice(h * BLK, (h + 1) * BLK)
            hi = slice((h + 1) * BLK, (h + 2) * BLK)
            outs.append(
                jnp.where(value_side, mixed[hi], swapped[lo])
                / jnp.where(value_side, swapped[hi], mixed[lo])
            )
        return jnp.concatenate(outs, axis=1).astype(jnp.bfloat16)

    def piece(owner, k):
        return full.at[owner, pl.ds(k * BLK, BLK)]

    def near(way, k):
        return pltpu.make_async_remote_copy(
            piece(t, k), piece(t, k), tp_send.at[way, k], tp_recv.at[way, k],
            device_id={"tp": (right, left)[way]}, device_id_type=MESH,
        )

    def onward(k):
        way = k % 2
        source = (left, right)[way]
        return pltpu.make_async_remote_copy(
            piece(source, k), piece(source, k), tp_send.at[2, k], tp_recv.at[2, k],
            device_id={"tp": (right, left)[way]}, device_id_type=MESH,
        )

    def pass_on(k):
        near(k % 2, k).wait_recv()
        onward(k).start()

    for b in range(blocks):
        full[t, pl.ds(b * BLK, BLK)] = attend_block(b)
        near(0, b).start()
        near(1, b).start()
    for b in range(blocks):
        pass_on(b)

    width = heads * HD
    for k in range(row_count // out_rows):
        for b in range(k * out_rows // BLK, (k + 1) * out_rows // BLK):
            near((b + 1) % 2, b).wait_recv()
            onward(b).wait_recv()
        total = None
        squares = None
        for owner in range(nt):
            wide = full[owner, pl.ds(k * out_rows, out_rows)].astype(jnp.float32)
            square = jnp.sum(wide * wide, axis=1, keepdims=True)
            scaled = (wide * gain_ref[:, pl.ds(owner * width, width)]).astype(jnp.bfloat16)
            term = jnp.dot(
                scaled,
                w_out[pl.ds(owner * width, width), :],
                preferred_element_type=jnp.float32,
            )
            total = term if total is None else total + term
            squares = square if squares is None else squares + square
        inverse = lax.rsqrt(squares / (HQ * HD) + norm_eps)
        out_ref[pl.ds(k * out_rows, out_rows), :] = (inverse * total).astype(jnp.bfloat16)

    for copy in hops.values():
        copy.wait_send()
    sends = wall.at[pl.ds(0, rows + cols - 2)]
    pltpu.make_async_copy(sends, sends, want_send).wait()

    @pl.loop(1, rows)
    def _(d):
        for g in range(len(groups_a)):
            @pl.when(needed_a(g))
            def _():
                send_a(d, g).wait_send()

    @pl.loop(1, cols)
    def _(d):
        for g in range(len(groups_b)):
            later, copy = send_b(d, g)

            @pl.when(later)
            def _():
                copy.wait_send()

    for k in range(blocks):
        near(0, k).wait_send()
        near(1, k).wait_send()
        onward(k).wait_send()


def per_device(tokens, w_query, w_key, w_value, w_out, out_gain, chosen):
    nz, ny, nt = lax.axis_size("kv_0"), lax.axis_size("kv_1"), lax.axis_size("tp")
    row_count, depth = tokens.shape
    blocks = row_count // BLK
    heads = w_query.shape[1] // HD
    rows, cols = ny * CORES, nz * CORES
    half_size = HD // 2
    frequency = np.float64(rope_base) ** (-np.arange(half_size) / half_size)
    frequency = jnp.asarray(np.tile(frequency, 4)[None, :], jnp.float32)

    piece = (HALF, 2 * HD)
    vmem = pl.BlockSpec(memory_space=pltpu.VMEM)
    far = pl.BlockSpec(memory_space=pltpu.HBM)
    dma = pltpu.SemaphoreType.DMA
    bf16 = jnp.bfloat16
    steps = max(nz, ny) // 2
    return pl.pallas_call(
        functools.partial(layer_kernel, nz, ny, nt),
        out_shape=jax.ShapeDtypeStruct((row_count, w_out.shape[1]), bf16),
        in_specs=[far] * 8,
        out_specs=vmem,
        scratch_shapes=[
            pltpu.VMEM(chosen.shape[1:], jnp.int32),
            pltpu.SMEM(chosen.shape[1:], jnp.int32),
            pltpu.VMEM((1, out_gain.shape[0]), jnp.float32),
            pltpu.VMEM((1, 2 * HD), jnp.float32),
            pltpu.VMEM((BLK + blocks, 2 * HD), jnp.float32),
            pltpu.VMEM((BLK + blocks, 2 * HD), jnp.float32),
            pltpu.VMEM((row_count, depth), bf16),
            pltpu.VMEM((2 * HD, depth), bf16),
            pltpu.VMEM(w_query.shape, bf16),
            pltpu.VMEM(w_out.shape, bf16),
            pltpu.VMEM((2, blocks, *piece), bf16),
            pltpu.VMEM((heads, row_count, 2 * HD), bf16),
            [pltpu.VMEM((blocks, *piece), bf16)] * (nz - 1),
            [pltpu.VMEM((blocks, *piece), bf16)] * (ny - 1),
            pltpu.VMEM((rows, nz, *piece), bf16),
            pltpu.VMEM((cols, ny, *piece), bf16),
            pltpu.VMEM((rows, nz, *piece), bf16),
            pltpu.VMEM((cols, ny, *piece), bf16),
            pltpu.VMEM((1, 128), jnp.int32),
            pltpu.VMEM((rows + cols, 1, 128), jnp.int32),
            pltpu.SMEM((rows + cols, 1, 128), jnp.int32),
            pltpu.VMEM((blocks, SEL * BLK, 2 * HD), bf16),
            pltpu.VMEM((nt, row_count, heads * HD), bf16),
            dma((9,)),
            dma, dma, dma,
            dma((2, 2, steps)),
            dma((2, 2, steps)),
            dma((4, rows)),
            dma((4, rows)),
            dma((4, cols)),
            dma((4, cols)),
            dma((3, blocks)),
            dma((3, blocks)),
        ],
        compiler_params=pltpu.CompilerParams(collective_id=0, has_side_effects=True, vmem_limit_bytes=40*2**20),
    )(
        *(
            pltpu.with_memory_space_constraint(a, pltpu.HBM)
            for a in (
                chosen[0], out_gain[None, :], frequency,
                tokens, w_key.T, w_value.T, w_query, w_out,
            )
        )
    )


def solution(mesh):
    count = mesh.shape["kv"]
    ny = 8 if count == 128 else 2
    nz = count // (ny * CORES)
    finer = Mesh(
        mesh.devices.reshape(nz, ny, CORES, mesh.shape["tp"]), ("kv_0", "kv_1", "kv_2", "tp")
    )
    placed = (
        P(KV, None),
        P(None, "tp"),
        P(None, "tp"),
        P(None, "tp"),
        P(None, "tp"),
        P(),
        P("tp", KV, None),
    )
    return jax.shard_map(
        per_device, mesh=finer, in_specs=placed, out_specs=P(KV, "tp"), check_vma=False
    )
```

```python
import functools

import jax
import jax.numpy as jnp
import numpy as np
from jax import lax
from jax.experimental import pallas as pl
from jax.experimental.pallas import tpu as pltpu
from jax.sharding import Mesh
from jax.sharding import PartitionSpec as P

HQ = 16
HD = 64
BLK = 64
SEL = 8
HALF = BLK // 2
CORES = 2
KV = ("kv_0", "kv_1", "kv_2")
MESH = pl.DeviceIdType.MESH

rope_base = 500000.0
norm_eps = 1e-06


def layer_kernel(
    nz, ny, nt,
    chosen_hbm, gain_hbm, frequency_hbm, tokens_hbm, wk_hbm, wv_hbm, wq_hbm, wo_hbm, out_ref,
    ids_ref, chosen_ref, gain_ref, frequency_ref, cos_ref, sin_ref,
    tokens, w_pair, w_query, w_out, pairs, query, ga, gb, sa, sb, ra, rb, want, wall, wsm, kv, full,
    load_sem, want_send, want_recv, smem_sem, ring_send, ring_recv,
    a_send, a_recv, b_send, b_recv, tp_send, tp_recv,
):
    z, y, c = lax.axis_index("kv_0"), lax.axis_index("kv_1"), lax.axis_index("kv_2")
    t = lax.axis_index("tp")
    rows, cols = ny * CORES, nz * CORES
    row_me, col_me = y * CORES + c, z * CORES + c
    blocks = pairs.shape[1]
    me = z * rows + row_me
    heads, row_count = query.shape[0], query.shape[1]

    def row_peer(d):
        p = lax.rem(row_me + d, rows)
        return p, {"kv_0": z, "kv_1": p // CORES, "kv_2": lax.rem(p, CORES)}

    def col_peer(d):
        p = lax.rem(col_me + d, cols)
        return p, {"kv_0": p // CORES, "kv_1": y, "kv_2": lax.rem(p, CORES)}

    right, left = lax.rem(t + 1, nt), lax.rem(t + nt - 1, nt)
    barrier = pltpu.get_barrier_semaphore()

    @pl.loop(1, rows)
    def _(d):
        _, peer = row_peer(d)
        pl.semaphore_signal(barrier, inc=1, device_id=peer, device_id_type=MESH)

    @pl.loop(1, nz)
    def _(d):
        for core in range(CORES):
            peer = {"kv_0": lax.rem(z + d, nz), "kv_1": y, "kv_2": core}
            pl.semaphore_signal(barrier, inc=1, device_id=peer, device_id_type=MESH)

    for peer in (right, left):
        pl.semaphore_signal(barrier, inc=1, device_id={"tp": peer}, device_id_type=MESH)

    loads = [
        pltpu.make_async_copy(source, target, load_sem.at[k])
        for k, (source, target) in enumerate(
            (
                (chosen_hbm, ids_ref),
                (frequency_hbm, frequency_ref),
                (wk_hbm, w_pair.at[pl.ds(0, HD)]),
                (wv_hbm, w_pair.at[pl.ds(HD, HD)]),
                (tokens_hbm, tokens),
                (wq_hbm, w_query),
                (wo_hbm, w_out),
                (gain_hbm, gain_ref),
                (chosen_hbm, chosen_ref),
            )
        )
    ]
    for load in loads:
        load.start()

    head_lane = lax.broadcasted_iota(jnp.int32, (1, 2 * HD), 1)
    value_side = head_lane >= HD
    lower_side = head_lane % HD < HD // 2
    loads[0].wait()
    loads[1].wait()
    place = lax.broadcasted_iota(jnp.int32, (BLK + blocks, 2 * HD), 0)
    place = jnp.where(place < BLK, place, (me * blocks + place - BLK) * BLK)
    angles = place.astype(jnp.float32) * frequency_ref[...]
    cos_ref[...] = jnp.cos(angles)
    sin_ref[...] = jnp.sin(angles) * jnp.where(lower_side, -1.0, 1.0)

    lane = lax.broadcasted_iota(jnp.int32, (blocks, 128), 1)
    found = jnp.full((blocks, 128), -1, jnp.int32)
    for s in range(SEL):
        ids = jnp.broadcast_to(ids_ref[:, s : s + 1], (blocks, 128))
        hit = (ids // blocks == lane) & (ids >= 0) & (lane != me)
        found = jnp.maximum(found, jnp.where(hit, ids % blocks, -1))
    want[...] = jnp.max(found, axis=0, keepdims=True)

    def turned(wide, b, only_keys):
        cos_row, sin_row = cos_ref[pl.ds(0, BLK)], sin_ref[pl.ds(0, BLK)]
        cos_base, sin_base = cos_ref[pl.ds(BLK + b, 1)], sin_ref[pl.ds(BLK + b, 1)]
        cosine = cos_base * cos_row - sin_base * sin_row
        sine_wave = sin_base * cos_row + cos_base * sin_row
        if only_keys:
            cosine = jnp.where(value_side, 1.0, cosine)
            sine_wave = jnp.where(value_side, 0.0, sine_wave)
        other = jnp.where(lower_side, pltpu.roll(wide, 3 * HD // 2, 1), pltpu.roll(wide, HD // 2, 1))
        return wide * cosine + other * sine_wave

    for load in loads[2:5]:
        load.wait()
    pair = lax.dot_general(
        tokens[...], w_pair[...], (((1,), (1,)), ((), ())), preferred_element_type=jnp.float32
    )
    for b in range(blocks):
        held = turned(pair[b * BLK : (b + 1) * BLK], b, True).astype(jnp.bfloat16)
        pairs[0, b] = held[:HALF]
        pairs[1, b] = held[HALF:]

    pl.semaphore_wait(barrier, rows - 1 + (nz - 1) * CORES + 2)

    pltpu.make_async_copy(want, wall.at[row_me], want_recv).start()
    pltpu.make_async_copy(want, wall.at[rows + col_me], want_recv).start()

    @pl.loop(1, rows)
    def _(d):
        _, peer = row_peer(d)
        pltpu.make_async_remote_copy(
            want, wall.at[row_me], want_send, want_recv, device_id=peer, device_id_type=MESH
        ).start()

    @pl.loop(1, cols)
    def _(d):
        _, peer = col_peer(d)
        pltpu.make_async_remote_copy(
            want, wall.at[rows + col_me], want_send, want_recv, device_id=peer, device_id_type=MESH
        ).start()

    def ring_copy(axis, way, step):
        name, place, size, held = (("kv_0", z, nz, ga), ("kv_1", y, ny, gb))[axis]
        target = lax.rem(place + (1, size - 1)[way], size)
        return pltpu.make_async_remote_copy(
            pairs.at[axis] if step == 0 else held[2 * step - 2 + way],
            held[2 * step + way],
            ring_send.at[axis, way, step],
            ring_recv.at[axis, way, step],
            device_id={name: target},
            device_id_type=MESH,
        )

    def source_of(place, size, k):
        if k % 2:
            return lax.rem(place - (k + 1) // 2 + size, size)
        return lax.rem(place + k // 2, size)

    def groups_of(size):
        found = [(0, 1)]
        for s in range(1, size // 2 + 1):
            found.append((2 * s - 1, min(2 * s + 1, size)))
        if size >= 8:
            found[-2:] = [(found[-2][0], found[-1][1])]
        return found

    def sent_at(group):
        return min(group[1] // 2 + 1, last)

    groups_a, groups_b = groups_of(nz), groups_of(ny)

    def send_a(d, g):
        p, peer = row_peer(d)
        lo, hi = groups_a[g]
        part = pl.ds(lo, hi - lo)
        return pltpu.make_async_remote_copy(
            sa.at[p, part], ra.at[row_me, part], a_send.at[g, p], a_recv.at[g, row_me],
            device_id=peer, device_id_type=MESH,
        )

    def send_b(d, g):
        p, peer = col_peer(d)
        lo, hi = groups_b[g]
        part = pl.ds(lo, hi - lo)
        copy = pltpu.make_async_remote_copy(
            sb.at[p, part], rb.at[col_me, part], b_send.at[g, p], b_recv.at[g, col_me],
            device_id=peer, device_id_type=MESH,
        )
        return p // CORES >= z, copy

    def needed_a(g):
        return z >= (groups_a[g][0] + 1) // 2

    def select_a(g):
        @pl.when(needed_a(g))
        def _():
            @pl.loop(0, rows)
            def _(p):
                for k in range(*groups_a[g]):
                    source = source_of(z, nz, k)
                    block = jnp.maximum(wsm[p, 0, source * rows + row_me], 0)
                    sa[p, k] = pairs[0, block] if k == 0 else ga[k - 1][block]

    def select_b(g):
        @pl.loop(0, cols)
        def _(p):
            for k in range(*groups_b[g]):
                source = source_of(y, ny, k)
                block = jnp.maximum(wsm[rows + p, 0, z * rows + source * CORES + c], 0)
                sb[p, k] = pairs[1, block] if k == 0 else gb[k - 1][block]

    def start_a(g):
        lo, hi = groups_a[g]
        part = pl.ds(lo, hi - lo)

        @pl.when(needed_a(g))
        def _():
            if g == 0:
                @pl.loop(1, rows - row_me)
                def _(d):
                    send_a(d, g).start()
            else:
                @pl.loop(1, rows)
                def _(d):
                    send_a(d, g).start()

            pltpu.make_async_copy(
                sa.at[row_me, part], ra.at[row_me, part], a_recv.at[g, row_me]
            ).start()

    def start_b(g):
        lo, hi = groups_b[g]
        part = pl.ds(lo, hi - lo)

        @pl.loop(1, cols)
        def _(d):
            later, copy = send_b(d, g)

            @pl.when(later)
            def _():
                copy.start()

        pltpu.make_async_copy(
            sb.at[col_me, part], rb.at[col_me, part], b_recv.at[g, col_me]
        ).start()

    hops = {}
    last = max(nz, ny) // 2

    def ring_step(step):
        for axis, size in ((1, ny), (0, nz)):
            for way, count in ((0, size // 2), (1, (size - 1) // 2)):
                if 0 < step <= count:
                    hops[axis, way, step - 1].wait_recv()
                if step < count:
                    hops[axis, way, step] = ring_copy(axis, way, step)
                    hops[axis, way, step].start()

    ring_step(0)
    ring_step(1)
    pltpu.make_async_copy(wall, wall, want_recv).wait()
    to_smem = pltpu.make_async_copy(wall, wsm, smem_sem)
    to_smem.start()
    to_smem.wait()
    for step in range(1, last + 1):
        if step > 1:
            ring_step(step)
        now_a = [g for g, group in enumerate(groups_a) if sent_at(group) == step]
        now_b = [g for g, group in enumerate(groups_b) if sent_at(group) == step]
        for g in now_a:
            select_a(g)
        for g in now_b:
            select_b(g)
        for g in now_a:
            start_a(g)
        for g in now_b:
            start_b(g)

    loads[5].wait()
    product = jnp.dot(tokens[...], w_query[...], preferred_element_type=jnp.float32)
    for b in range(blocks):
        for h in range(0, heads, 2):
            wide = product[b * BLK : (b + 1) * BLK, h * HD : (h + 2) * HD]
            wide = turned(wide, b, False) * (HD ** -0.5)
            spot = pl.ds(b * BLK, BLK)
            query[h, spot] = jnp.where(value_side, 0.0, wide).astype(jnp.bfloat16)
            query[h + 1, spot] = jnp.where(
                value_side, 0.0, pltpu.roll(wide, HD, 1)
            ).astype(jnp.bfloat16)
    for load in loads[6:]:
        load.wait()

    @pl.loop(0, rows)
    def _(p):
        for g, (lo, hi) in enumerate(groups_a):
            part = pl.ds(lo, hi - lo)

            @pl.when(p <= row_me if g == 0 else needed_a(g))
            def _():
                pltpu.make_async_copy(sa.at[p, part], ra.at[p, part], a_recv.at[g, p]).wait()

    @pl.loop(0, cols)
    def _(p):
        @pl.when(p // CORES <= z)
        def _():
            for g, (lo, hi) in enumerate(groups_b):
                part = pl.ds(lo, hi - lo)
                pltpu.make_async_copy(sb.at[p, part], rb.at[p, part], b_recv.at[g, p]).wait()

    out_rows = 2 * BLK
    key_lane = lax.broadcasted_iota(jnp.int32, (1, SEL * BLK), 1)
    query_row = lax.broadcasted_iota(jnp.int32, (BLK, SEL * BLK), 0)
    key_col = lax.broadcasted_iota(jnp.int32, (BLK, SEL * BLK), 1)
    causal = jnp.where((key_col < BLK) & (key_col > query_row), -jnp.inf, 0.0).astype(jnp.float32)

    def slot_of(place, size, owner):
        r = lax.rem(place - owner + size, size)
        return jnp.where(r <= size // 2, jnp.maximum(2 * r - 1, 0), 2 * (size - r))

    def attend_block(b):
        bias = jnp.zeros((1, SEL * BLK), jnp.float32)
        for s in range(SEL):
            named = chosen_ref[b, s]
            owner = lax.shift_right_arithmetic(named, 3)
            index = lax.bitwise_and(named, blocks - 1)
            here = (named < 0) | (owner == me)
            owner = jnp.where(here, me, owner)
            oz, oy, oc = owner // rows, lax.rem(owner, rows) // CORES, lax.rem(owner, CORES)
            kv[b, pl.ds(s * BLK, HALF)] = jnp.where(
                here, pairs[0, index], ra[oy * CORES + oc, slot_of(z, nz, oz)]
            )
            kv[b, pl.ds(s * BLK + HALF, HALF)] = jnp.where(
                here, pairs[1, index], rb[oz * CORES + oc, slot_of(y, ny, oy)]
            )
            if s > 0:
                bias = jnp.where((key_lane // BLK == s) & (named < 0), -jnp.inf, bias)
        keys = kv[b]
        queries = query[:, pl.ds(b * BLK, BLK), :].reshape(heads * BLK, 2 * HD)
        scores = lax.dot_general(
            queries, keys, (((1,), (1,)), ((), ())), preferred_element_type=jnp.float32
        )
        scores = scores.reshape(heads, BLK, SEL * BLK) + (causal + bias)[None]
        scores = scores.reshape(heads * BLK, SEL * BLK)
        peak = jnp.max(scores, axis=1, keepdims=True)
        weights = jnp.exp(scores - peak).astype(jnp.bfloat16)
        ones_or_values = jnp.where(value_side, keys, jnp.ones((), jnp.bfloat16))
        mixed = jnp.dot(weights, ones_or_values, preferred_element_type=jnp.float32)
        swapped = pltpu.roll(mixed, HD, 1)
        outs = []
        for h in range(0, heads, 2):
            lo = slice(h * BLK, (h + 1) * BLK)
            hi = slice((h + 1) * BLK, (h + 2) * BLK)
            outs.append(
                jnp.where(value_side, mixed[hi], swapped[lo])
                / jnp.where(value_side, swapped[hi], mixed[lo])
            )
        return jnp.concatenate(outs, axis=1).astype(jnp.bfloat16)

    def piece(owner, k):
        return full.at[owner, pl.ds(k * BLK, BLK)]

    def near(way, k):
        return pltpu.make_async_remote_copy(
            piece(t, k), piece(t, k), tp_send.at[way, k], tp_recv.at[way, k],
            device_id={"tp": (right, left)[way]}, device_id_type=MESH,
        )

    def onward(k):
        way = k % 2
        source = (left, right)[way]
        return pltpu.make_async_remote_copy(
            piece(source, k), piece(source, k), tp_send.at[2, k], tp_recv.at[2, k],
            device_id={"tp": (right, left)[way]}, device_id_type=MESH,
        )

    def pass_on(k):
        near(k % 2, k).wait_recv()
        onward(k).start()

    for b in range(blocks):
        full[t, pl.ds(b * BLK, BLK)] = attend_block(b)
        near(0, b).start()
        near(1, b).start()
    for b in range(blocks):
        pass_on(b)

    width = heads * HD
    for k in range(row_count // out_rows):
        for b in range(k * out_rows // BLK, (k + 1) * out_rows // BLK):
            near((b + 1) % 2, b).wait_recv()
            onward(b).wait_recv()
        total = None
        squares = None
        for owner in range(nt):
            wide = full[owner, pl.ds(k * out_rows, out_rows)].astype(jnp.float32)
            square = jnp.sum(wide * wide, axis=1, keepdims=True)
            scaled = (wide * gain_ref[:, pl.ds(owner * width, width)]).astype(jnp.bfloat16)
            term = jnp.dot(
                scaled,
                w_out[pl.ds(owner * width, width), :],
                preferred_element_type=jnp.float32,
            )
            total = term if total is None else total + term
            squares = square if squares is None else squares + square
        inverse = lax.rsqrt(squares / (HQ * HD) + norm_eps)
        out_ref[pl.ds(k * out_rows, out_rows), :] = (inverse * total).astype(jnp.bfloat16)

    for copy in hops.values():
        copy.wait_send()
    sends = wall.at[pl.ds(0, rows + cols - 2)]
    pltpu.make_async_copy(sends, sends, want_send).wait()

    @pl.loop(1, rows)
    def _(d):
        for g in range(len(groups_a)):
            @pl.when(d < rows - row_me if g == 0 else needed_a(g))
            def _():
                send_a(d, g).wait_send()

    @pl.loop(1, cols)
    def _(d):
        for g in range(len(groups_b)):
            later, copy = send_b(d, g)

            @pl.when(later)
            def _():
                copy.wait_send()

    for k in range(blocks):
        near(0, k).wait_send()
        near(1, k).wait_send()
        onward(k).wait_send()


def per_device(tokens, w_query, w_key, w_value, w_out, out_gain, chosen):
    nz, ny, nt = lax.axis_size("kv_0"), lax.axis_size("kv_1"), lax.axis_size("tp")
    row_count, depth = tokens.shape
    blocks = row_count // BLK
    heads = w_query.shape[1] // HD
    rows, cols = ny * CORES, nz * CORES
    half_size = HD // 2
    frequency = np.float64(rope_base) ** (-np.arange(half_size) / half_size)
    frequency = jnp.asarray(np.tile(frequency, 4)[None, :], jnp.float32)

    piece = (HALF, 2 * HD)
    vmem = pl.BlockSpec(memory_space=pltpu.VMEM)
    far = pl.BlockSpec(memory_space=pltpu.HBM)
    dma = pltpu.SemaphoreType.DMA
    bf16 = jnp.bfloat16
    steps = max(nz, ny) // 2
    return pl.pallas_call(
        functools.partial(layer_kernel, nz, ny, nt),
        out_shape=jax.ShapeDtypeStruct((row_count, w_out.shape[1]), bf16),
        in_specs=[far] * 8,
        out_specs=vmem,
        scratch_shapes=[
            pltpu.VMEM(chosen.shape[1:], jnp.int32),
            pltpu.SMEM(chosen.shape[1:], jnp.int32),
            pltpu.VMEM((1, out_gain.shape[0]), jnp.float32),
            pltpu.VMEM((1, 2 * HD), jnp.float32),
            pltpu.VMEM((BLK + blocks, 2 * HD), jnp.float32),
            pltpu.VMEM((BLK + blocks, 2 * HD), jnp.float32),
            pltpu.VMEM((row_count, depth), bf16),
            pltpu.VMEM((2 * HD, depth), bf16),
            pltpu.VMEM(w_query.shape, bf16),
            pltpu.VMEM(w_out.shape, bf16),
            pltpu.VMEM((2, blocks, *piece), bf16),
            pltpu.VMEM((heads, row_count, 2 * HD), bf16),
            [pltpu.VMEM((blocks, *piece), bf16)] * (nz - 1),
            [pltpu.VMEM((blocks, *piece), bf16)] * (ny - 1),
            pltpu.VMEM((rows, nz, *piece), bf16),
            pltpu.VMEM((cols, ny, *piece), bf16),
            pltpu.VMEM((rows, nz, *piece), bf16),
            pltpu.VMEM((cols, ny, *piece), bf16),
            pltpu.VMEM((1, 128), jnp.int32),
            pltpu.VMEM((rows + cols, 1, 128), jnp.int32),
            pltpu.SMEM((rows + cols, 1, 128), jnp.int32),
            pltpu.VMEM((blocks, SEL * BLK, 2 * HD), bf16),
            pltpu.VMEM((nt, row_count, heads * HD), bf16),
            dma((9,)),
            dma, dma, dma,
            dma((2, 2, steps)),
            dma((2, 2, steps)),
            dma((4, rows)),
            dma((4, rows)),
            dma((4, cols)),
            dma((4, cols)),
            dma((3, blocks)),
            dma((3, blocks)),
        ],
        compiler_params=pltpu.CompilerParams(collective_id=0, has_side_effects=True, vmem_limit_bytes=40*2**20),
    )(
        *(
            pltpu.with_memory_space_constraint(a, pltpu.HBM)
            for a in (
                chosen[0], out_gain[None, :], frequency,
                tokens, w_key.T, w_value.T, w_query, w_out,
            )
        )
    )


def solution(mesh):
    count = mesh.shape["kv"]
    ny = 8 if count == 128 else 2
    nz = count // (ny * CORES)
    finer = Mesh(
        mesh.devices.reshape(nz, ny, CORES, mesh.shape["tp"]), ("kv_0", "kv_1", "kv_2", "tp")
    )
    placed = (
        P(KV, None),
        P(None, "tp"),
        P(None, "tp"),
        P(None, "tp"),
        P(None, "tp"),
        P(),
        P("tp", KV, None),
    )
    return jax.shard_map(
        per_device, mesh=finer, in_specs=placed, out_specs=P(KV, "tp"), check_vma=False
    )
```

```python
import functools

import jax
import jax.numpy as jnp
import numpy as np
from jax import lax
from jax.experimental import pallas as pl
from jax.experimental.pallas import tpu as pltpu
from jax.sharding import Mesh
from jax.sharding import PartitionSpec as P

HQ = 16
HD = 64
BLK = 64
SEL = 8
HALF = BLK // 2
CORES = 2
KV = ("kv_0", "kv_1", "kv_2")
MESH = pl.DeviceIdType.MESH

rope_base = 500000.0
norm_eps = 1e-06


def layer_kernel(
    nz, ny, nt,
    chosen_hbm, gain_hbm, frequency_hbm, tokens_hbm, wk_hbm, wv_hbm, wq_hbm, wo_hbm, out_ref,
    ids_ref, chosen_ref, gain_ref, frequency_ref, cos_ref, sin_ref,
    tokens, w_pair, w_query, w_out, pairs, query, ga, gb, sa, sb, ra, rb, want, wall, wsm, kv, full,
    load_sem, want_send, want_recv, smem_sem, ring_send, ring_recv,
    a_send, a_recv, b_send, b_recv, tp_send, tp_recv,
):
    z, y, c = lax.axis_index("kv_0"), lax.axis_index("kv_1"), lax.axis_index("kv_2")
    t = lax.axis_index("tp")
    rows, cols = ny * CORES, nz * CORES
    row_me, col_me = y * CORES + c, z * CORES + c
    blocks = pairs.shape[1]
    me = z * rows + row_me
    heads, row_count = query.shape[0], query.shape[1]

    def row_peer(d):
        p = lax.rem(row_me + d, rows)
        return p, {"kv_0": z, "kv_1": p // CORES, "kv_2": lax.rem(p, CORES)}

    def col_peer(d):
        p = lax.rem(col_me + d, cols)
        return p, {"kv_0": p // CORES, "kv_1": y, "kv_2": lax.rem(p, CORES)}

    right, left = lax.rem(t + 1, nt), lax.rem(t + nt - 1, nt)
    barrier = pltpu.get_barrier_semaphore()

    @pl.loop(1, rows)
    def _(d):
        _, peer = row_peer(d)
        pl.semaphore_signal(barrier, inc=1, device_id=peer, device_id_type=MESH)

    @pl.loop(1, nz)
    def _(d):
        for core in range(CORES):
            peer = {"kv_0": lax.rem(z + d, nz), "kv_1": y, "kv_2": core}
            pl.semaphore_signal(barrier, inc=1, device_id=peer, device_id_type=MESH)

    for peer in (right, left):
        pl.semaphore_signal(barrier, inc=1, device_id={"tp": peer}, device_id_type=MESH)

    loads = [
        pltpu.make_async_copy(source, target, load_sem.at[k])
        for k, (source, target) in enumerate(
            (
                (chosen_hbm, ids_ref),
                (frequency_hbm, frequency_ref),
                (wk_hbm, w_pair.at[pl.ds(0, HD)]),
                (wv_hbm, w_pair.at[pl.ds(HD, HD)]),
                (tokens_hbm, tokens),
                (wq_hbm, w_query),
                (wo_hbm, w_out),
                (gain_hbm, gain_ref),
                (chosen_hbm, chosen_ref),
            )
        )
    ]
    for load in loads:
        load.start()

    head_lane = lax.broadcasted_iota(jnp.int32, (1, 2 * HD), 1)
    value_side = head_lane >= HD
    lower_side = head_lane % HD < HD // 2
    loads[0].wait()
    loads[1].wait()
    place = lax.broadcasted_iota(jnp.int32, (BLK + blocks, 2 * HD), 0)
    place = jnp.where(place < BLK, place, (me * blocks + place - BLK) * BLK)
    angles = place.astype(jnp.float32) * frequency_ref[...]
    cos_ref[...] = jnp.cos(angles)
    sin_ref[...] = jnp.sin(angles) * jnp.where(lower_side, -1.0, 1.0)

    lane = lax.broadcasted_iota(jnp.int32, (blocks, 128), 1)
    found = jnp.full((blocks, 128), -1, jnp.int32)
    for s in range(SEL):
        ids = jnp.broadcast_to(ids_ref[:, s : s + 1], (blocks, 128))
        hit = (ids // blocks == lane) & (ids >= 0) & (lane != me)
        found = jnp.maximum(found, jnp.where(hit, ids % blocks, -1))
    want[...] = jnp.max(found, axis=0, keepdims=True)

    def turned(wide, b, only_keys):
        cos_row, sin_row = cos_ref[pl.ds(0, BLK)], sin_ref[pl.ds(0, BLK)]
        cos_base, sin_base = cos_ref[pl.ds(BLK + b, 1)], sin_ref[pl.ds(BLK + b, 1)]
        cosine = cos_base * cos_row - sin_base * sin_row
        sine_wave = sin_base * cos_row + cos_base * sin_row
        if only_keys:
            cosine = jnp.where(value_side, 1.0, cosine)
            sine_wave = jnp.where(value_side, 0.0, sine_wave)
        other = jnp.where(lower_side, pltpu.roll(wide, 3 * HD // 2, 1), pltpu.roll(wide, HD // 2, 1))
        return wide * cosine + other * sine_wave

    for load in loads[2:5]:
        load.wait()
    pair = lax.dot_general(
        tokens[...], w_pair[...], (((1,), (1,)), ((), ())), preferred_element_type=jnp.float32
    )
    for b in range(blocks):
        held = turned(pair[b * BLK : (b + 1) * BLK], b, True).astype(jnp.bfloat16)
        pairs[0, b] = held[:HALF]
        pairs[1, b] = held[HALF:]

    pl.semaphore_wait(barrier, rows - 1 + (nz - 1) * CORES + 2)

    pltpu.make_async_copy(want, wall.at[row_me], want_recv).start()
    pltpu.make_async_copy(want, wall.at[rows + col_me], want_recv).start()

    @pl.loop(1, rows)
    def _(d):
        _, peer = row_peer(d)
        pltpu.make_async_remote_copy(
            want, wall.at[row_me], want_send, want_recv, device_id=peer, device_id_type=MESH
        ).start()

    @pl.loop(1, cols)
    def _(d):
        _, peer = col_peer(d)
        pltpu.make_async_remote_copy(
            want, wall.at[rows + col_me], want_send, want_recv, device_id=peer, device_id_type=MESH
        ).start()

    def ring_copy(axis, way, step):
        name, place, size, held = (("kv_0", z, nz, ga), ("kv_1", y, ny, gb))[axis]
        target = lax.rem(place + (1, size - 1)[way], size)
        return pltpu.make_async_remote_copy(
            pairs.at[axis] if step == 0 else held[2 * step - 2 + way],
            held[2 * step + way],
            ring_send.at[axis, way, step],
            ring_recv.at[axis, way, step],
            device_id={name: target},
            device_id_type=MESH,
        )

    def source_of(place, size, k):
        if k % 2:
            return lax.rem(place - (k + 1) // 2 + size, size)
        return lax.rem(place + k // 2, size)

    def groups_of(size):
        found = [(0, 1)]
        for s in range(1, size // 2 + 1):
            found.append((2 * s - 1, min(2 * s + 1, size)))
        if size >= 8:
            found[-2:] = [(found[-2][0], found[-1][1])]
        return found

    def sent_at(group):
        return min(group[1] // 2 + 1, last)

    groups_a, groups_b = groups_of(nz), groups_of(ny)

    def send_a(d, g):
        p, peer = row_peer(d)
        lo, hi = groups_a[g]
        part = pl.ds(lo, hi - lo)
        return pltpu.make_async_remote_copy(
            sa.at[p, part], ra.at[row_me, part], a_send.at[g, p], a_recv.at[g, row_me],
            device_id=peer, device_id_type=MESH,
        )

    def send_b(d, g):
        p, peer = col_peer(d)
        lo, hi = groups_b[g]
        part = pl.ds(lo, hi - lo)
        copy = pltpu.make_async_remote_copy(
            sb.at[p, part], rb.at[col_me, part], b_send.at[g, p], b_recv.at[g, col_me],
            device_id=peer, device_id_type=MESH,
        )
        return p // CORES >= z, copy

    def needed_a(g):
        return z >= (groups_a[g][0] + 1) // 2

    def select_a(g):
        @pl.when(needed_a(g))
        def _():
            @pl.loop(0, rows)
            def _(p):
                for k in range(*groups_a[g]):
                    source = source_of(z, nz, k)
                    block = jnp.maximum(wsm[p, 0, source * rows + row_me], 0)
                    sa[p, k] = pairs[0, block] if k == 0 else ga[k - 1][block]

    def select_b(g):
        @pl.loop(0, cols)
        def _(p):
            for k in range(*groups_b[g]):
                source = source_of(y, ny, k)
                block = jnp.maximum(wsm[rows + p, 0, z * rows + source * CORES + c], 0)
                sb[p, k] = pairs[1, block] if k == 0 else gb[k - 1][block]

    def start_a(g):
        lo, hi = groups_a[g]
        part = pl.ds(lo, hi - lo)

        @pl.when(needed_a(g))
        def _():
            if g == 0:
                @pl.loop(1, rows - row_me)
                def _(d):
                    send_a(d, g).start()
            else:
                @pl.loop(1, rows)
                def _(d):
                    send_a(d, g).start()

            pltpu.make_async_copy(
                sa.at[row_me, part], ra.at[row_me, part], a_recv.at[g, row_me]
            ).start()

    def start_b(g):
        lo, hi = groups_b[g]
        part = pl.ds(lo, hi - lo)

        @pl.loop(1, cols)
        def _(d):
            later, copy = send_b(d, g)

            @pl.when(later)
            def _():
                copy.start()

        pltpu.make_async_copy(
            sb.at[col_me, part], rb.at[col_me, part], b_recv.at[g, col_me]
        ).start()

    hops = {}
    last = max(nz, ny) // 2

    def ring_step(step):
        for axis, size in ((1, ny), (0, nz)):
            for way, count in ((0, size // 2), (1, (size - 1) // 2)):
                if 0 < step <= count:
                    hops[axis, way, step - 1].wait_recv()
                if step < count:
                    hops[axis, way, step] = ring_copy(axis, way, step)
                    hops[axis, way, step].start()

    ring_step(0)
    ring_step(1)
    pltpu.make_async_copy(wall, wall, want_recv).wait()
    to_smem = pltpu.make_async_copy(wall, wsm, smem_sem)
    to_smem.start()
    to_smem.wait()
    for step in range(1, last + 1):
        if step > 1:
            ring_step(step)
        now_a = [g for g, group in enumerate(groups_a) if sent_at(group) == step]
        now_b = [g for g, group in enumerate(groups_b) if sent_at(group) == step]
        for g in now_a:
            select_a(g)
        for g in now_b:
            select_b(g)
        for g in now_a:
            start_a(g)
        for g in now_b:
            start_b(g)

    loads[5].wait()
    product = jnp.dot(tokens[...], w_query[...], preferred_element_type=jnp.float32)
    for b in range(blocks):
        for h in range(0, heads, 2):
            wide = product[b * BLK : (b + 1) * BLK, h * HD : (h + 2) * HD]
            wide = turned(wide, b, False) * (HD ** -0.5)
            spot = pl.ds(b * BLK, BLK)
            query[h, spot] = jnp.where(value_side, 0.0, wide).astype(jnp.bfloat16)
            query[h + 1, spot] = jnp.where(
                value_side, 0.0, pltpu.roll(wide, HD, 1)
            ).astype(jnp.bfloat16)
    for load in loads[6:]:
        load.wait()

    @pl.loop(0, rows)
    def _(p):
        for g, (lo, hi) in enumerate(groups_a):
            part = pl.ds(lo, hi - lo)

            @pl.when(p <= row_me if g == 0 else needed_a(g))
            def _():
                pltpu.make_async_copy(sa.at[p, part], ra.at[p, part], a_recv.at[g, p]).wait()

    @pl.loop(0, cols)
    def _(p):
        @pl.when(p // CORES <= z)
        def _():
            for g, (lo, hi) in enumerate(groups_b):
                part = pl.ds(lo, hi - lo)
                pltpu.make_async_copy(sb.at[p, part], rb.at[p, part], b_recv.at[g, p]).wait()

    out_rows = BLK
    key_lane = lax.broadcasted_iota(jnp.int32, (1, SEL * BLK), 1)
    query_row = lax.broadcasted_iota(jnp.int32, (BLK, SEL * BLK), 0)
    key_col = lax.broadcasted_iota(jnp.int32, (BLK, SEL * BLK), 1)
    causal = jnp.where((key_col < BLK) & (key_col > query_row), -jnp.inf, 0.0).astype(jnp.float32)

    def slot_of(place, size, owner):
        r = lax.rem(place - owner + size, size)
        return jnp.where(r <= size // 2, jnp.maximum(2 * r - 1, 0), 2 * (size - r))

    def attend_block(b):
        bias = jnp.zeros((1, SEL * BLK), jnp.float32)
        for s in range(SEL):
            named = chosen_ref[b, s]
            owner = lax.shift_right_arithmetic(named, 3)
            index = lax.bitwise_and(named, blocks - 1)
            here = (named < 0) | (owner == me)
            owner = jnp.where(here, me, owner)
            oz, oy, oc = owner // rows, lax.rem(owner, rows) // CORES, lax.rem(owner, CORES)
            kv[b, pl.ds(s * BLK, HALF)] = jnp.where(
                here, pairs[0, index], ra[oy * CORES + oc, slot_of(z, nz, oz)]
            )
            kv[b, pl.ds(s * BLK + HALF, HALF)] = jnp.where(
                here, pairs[1, index], rb[oz * CORES + oc, slot_of(y, ny, oy)]
            )
            if s > 0:
                bias = jnp.where((key_lane // BLK == s) & (named < 0), -jnp.inf, bias)
        keys = kv[b]
        queries = query[:, pl.ds(b * BLK, BLK), :].reshape(heads * BLK, 2 * HD)
        scores = lax.dot_general(
            queries, keys, (((1,), (1,)), ((), ())), preferred_element_type=jnp.float32
        )
        scores = scores.reshape(heads, BLK, SEL * BLK) + (causal + bias)[None]
        scores = scores.reshape(heads * BLK, SEL * BLK)
        peak = jnp.max(scores, axis=1, keepdims=True)
        weights = jnp.exp(scores - peak).astype(jnp.bfloat16)
        ones_or_values = jnp.where(value_side, keys, jnp.ones((), jnp.bfloat16))
        mixed = jnp.dot(weights, ones_or_values, preferred_element_type=jnp.float32)
        swapped = pltpu.roll(mixed, HD, 1)
        outs = []
        for h in range(0, heads, 2):
            lo = slice(h * BLK, (h + 1) * BLK)
            hi = slice((h + 1) * BLK, (h + 2) * BLK)
            outs.append(
                jnp.where(value_side, mixed[hi], swapped[lo])
                / jnp.where(value_side, swapped[hi], mixed[lo])
            )
        return jnp.concatenate(outs, axis=1).astype(jnp.bfloat16)

    def piece(owner, k):
        return full.at[owner, pl.ds(k * BLK, BLK)]

    def near(way, k):
        return pltpu.make_async_remote_copy(
            piece(t, k), piece(t, k), tp_send.at[way, k], tp_recv.at[way, k],
            device_id={"tp": (right, left)[way]}, device_id_type=MESH,
        )

    def onward(k):
        way = k % 2
        source = (left, right)[way]
        return pltpu.make_async_remote_copy(
            piece(source, k), piece(source, k), tp_send.at[2, k], tp_recv.at[2, k],
            device_id={"tp": (right, left)[way]}, device_id_type=MESH,
        )

    def pass_on(k):
        near(k % 2, k).wait_recv()
        onward(k).start()

    for b in range(blocks):
        full[t, pl.ds(b * BLK, BLK)] = attend_block(b)
        near(0, b).start()
        near(1, b).start()
    for b in range(blocks):
        pass_on(b)

    width = heads * HD
    for k in range(row_count // out_rows):
        for b in range(k * out_rows // BLK, (k + 1) * out_rows // BLK):
            near((b + 1) % 2, b).wait_recv()
            onward(b).wait_recv()
        total = None
        squares = None
        for owner in range(nt):
            wide = full[owner, pl.ds(k * out_rows, out_rows)].astype(jnp.float32)
            square = jnp.sum(wide * wide, axis=1, keepdims=True)
            scaled = (wide * gain_ref[:, pl.ds(owner * width, width)]).astype(jnp.bfloat16)
            term = jnp.dot(
                scaled,
                w_out[pl.ds(owner * width, width), :],
                preferred_element_type=jnp.float32,
            )
            total = term if total is None else total + term
            squares = square if squares is None else squares + square
        inverse = lax.rsqrt(squares / (HQ * HD) + norm_eps)
        out_ref[pl.ds(k * out_rows, out_rows), :] = (inverse * total).astype(jnp.bfloat16)

    for copy in hops.values():
        copy.wait_send()
    sends = wall.at[pl.ds(0, rows + cols - 2)]
    pltpu.make_async_copy(sends, sends, want_send).wait()

    @pl.loop(1, rows)
    def _(d):
        for g in range(len(groups_a)):
            @pl.when(d < rows - row_me if g == 0 else needed_a(g))
            def _():
                send_a(d, g).wait_send()

    @pl.loop(1, cols)
    def _(d):
        for g in range(len(groups_b)):
            later, copy = send_b(d, g)

            @pl.when(later)
            def _():
                copy.wait_send()

    for k in range(blocks):
        near(0, k).wait_send()
        near(1, k).wait_send()
        onward(k).wait_send()


def per_device(tokens, w_query, w_key, w_value, w_out, out_gain, chosen):
    nz, ny, nt = lax.axis_size("kv_0"), lax.axis_size("kv_1"), lax.axis_size("tp")
    row_count, depth = tokens.shape
    blocks = row_count // BLK
    heads = w_query.shape[1] // HD
    rows, cols = ny * CORES, nz * CORES
    half_size = HD // 2
    frequency = np.float64(rope_base) ** (-np.arange(half_size) / half_size)
    frequency = jnp.asarray(np.tile(frequency, 4)[None, :], jnp.float32)

    piece = (HALF, 2 * HD)
    vmem = pl.BlockSpec(memory_space=pltpu.VMEM)
    far = pl.BlockSpec(memory_space=pltpu.HBM)
    dma = pltpu.SemaphoreType.DMA
    bf16 = jnp.bfloat16
    steps = max(nz, ny) // 2
    return pl.pallas_call(
        functools.partial(layer_kernel, nz, ny, nt),
        out_shape=jax.ShapeDtypeStruct((row_count, w_out.shape[1]), bf16),
        in_specs=[far] * 8,
        out_specs=vmem,
        scratch_shapes=[
            pltpu.VMEM(chosen.shape[1:], jnp.int32),
            pltpu.SMEM(chosen.shape[1:], jnp.int32),
            pltpu.VMEM((1, out_gain.shape[0]), jnp.float32),
            pltpu.VMEM((1, 2 * HD), jnp.float32),
            pltpu.VMEM((BLK + blocks, 2 * HD), jnp.float32),
            pltpu.VMEM((BLK + blocks, 2 * HD), jnp.float32),
            pltpu.VMEM((row_count, depth), bf16),
            pltpu.VMEM((2 * HD, depth), bf16),
            pltpu.VMEM(w_query.shape, bf16),
            pltpu.VMEM(w_out.shape, bf16),
            pltpu.VMEM((2, blocks, *piece), bf16),
            pltpu.VMEM((heads, row_count, 2 * HD), bf16),
            [pltpu.VMEM((blocks, *piece), bf16)] * (nz - 1),
            [pltpu.VMEM((blocks, *piece), bf16)] * (ny - 1),
            pltpu.VMEM((rows, nz, *piece), bf16),
            pltpu.VMEM((cols, ny, *piece), bf16),
            pltpu.VMEM((rows, nz, *piece), bf16),
            pltpu.VMEM((cols, ny, *piece), bf16),
            pltpu.VMEM((1, 128), jnp.int32),
            pltpu.VMEM((rows + cols, 1, 128), jnp.int32),
            pltpu.SMEM((rows + cols, 1, 128), jnp.int32),
            pltpu.VMEM((blocks, SEL * BLK, 2 * HD), bf16),
            pltpu.VMEM((nt, row_count, heads * HD), bf16),
            dma((9,)),
            dma, dma, dma,
            dma((2, 2, steps)),
            dma((2, 2, steps)),
            dma((4, rows)),
            dma((4, rows)),
            dma((4, cols)),
            dma((4, cols)),
            dma((3, blocks)),
            dma((3, blocks)),
        ],
        compiler_params=pltpu.CompilerParams(collective_id=0, has_side_effects=True, vmem_limit_bytes=40*2**20),
    )(
        *(
            pltpu.with_memory_space_constraint(a, pltpu.HBM)
            for a in (
                chosen[0], out_gain[None, :], frequency,
                tokens, w_key.T, w_value.T, w_query, w_out,
            )
        )
    )


def solution(mesh):
    count = mesh.shape["kv"]
    ny = 8 if count == 128 else 2
    nz = count // (ny * CORES)
    finer = Mesh(
        mesh.devices.reshape(nz, ny, CORES, mesh.shape["tp"]), ("kv_0", "kv_1", "kv_2", "tp")
    )
    placed = (
        P(KV, None),
        P(None, "tp"),
        P(None, "tp"),
        P(None, "tp"),
        P(None, "tp"),
        P(),
        P("tp", KV, None),
    )
    return jax.shard_map(
        per_device, mesh=finer, in_specs=placed, out_specs=P(KV, "tp"), check_vma=False
    )
```
